32 devices in a mesh: grp: 2 (over y), fs: 4 (over z), tp: 4 (over x, core).
Axes of the slice: x: 2, y: 2, z: 4, core: 2. Of those that a mesh axis runs over, the one named last changes fastest.
Arguments:
- tokens: bfloat16 [4096, 2048], P(('grp', 'fs')), parts along dimension 0, may hold values from -6 to 6
- norm_in: bfloat16 [2048], replicated, may hold values from 0.099609375 to 1.8984375
- w_value: bfloat16 [2048, 2048], P('fs', 'tp'), may hold values from -0.125 to 0.125
- w_gate: bfloat16 [2048, 2048], P('fs', 'tp'), may hold values from -0.125 to 0.125
- conv_kernel: float32 [31, 2048], replicated, as said below
- ln_gain: bfloat16 [2048], replicated, may hold values from 0.099609375 to 1.8984375
- ln_shift: bfloat16 [2048], replicated, may hold values from -3 to 3
- w_out: bfloat16 [2048, 2048], P('tp', 'fs'), may hold values from -0.125 to 0.125
- norm_mlp: bfloat16 [2048], replicated, may hold values from 0.099609375 to 1.8984375
- w_up: bfloat16 [2048, 8192], P('fs', 'tp'), may hold values from -0.125 to 0.125
- w_down: bfloat16 [8192, 2048], P('tp', 'fs'), may hold values from -0.0625 to 0.0625
Outputs:
- layer_out: bfloat16 [4096, 2048], P(('grp', 'fs', 'tp')), parts along dimension 0
The draws below stay inside these ranges and needn't reach their ends.
There are 2 independent parts, one for each index of `grp`. The reference program is written for one: setup_inputs(seed, part) draws one part's arguments, and reference() takes and returns one part's arrays. A program takes and returns all parts, laid end to end along the dimension named above; an argument that names none is the same for every part. Nothing has to cross between parts.
Inputs may be any that keep to these rules, and one draw needn't show every extreme that they name: `conv_kernel`: a depthwise kernel.
All inputs are finite; a program needn't handle non-finite values.
Results may differ from the reference program's by a relative error of at most 0.018.
Values may be sent and summed in bfloat16 or wider, within the bound.
A program may use at most 64 MiB of HBM per device.

```python
import jax
import jax.numpy as jnp
from jax import lax

D = 2048
FF = 8192
KERNEL = 31
SEQ = 512
TOKENS = 2048
N_FS = 4
N_TP = 4


def draw_conv_kernel(key, part):
    first, second = jax.random.split(jax.random.fold_in(key, 11), 2)
    base = jnp.clip(jax.random.normal(first, (KERNEL, D), jnp.float32), -4.0, 4.0) / jnp.sqrt(jnp.float32(KERNEL))
    channel = jnp.arange(D, dtype=jnp.float32) / D
    rising = jnp.exp(jnp.log(3.0) * channel) * jax.random.uniform(second, (D,), jnp.float32, 0.6, 1.4)
    return (base * rising[None, :]).astype(jnp.float32)


def block_scale(key, shape, cuts, low, high):
    def one(position, blocks):
        draws = jax.random.uniform(jax.random.fold_in(jax.random.fold_in(key, 6), position), (blocks,), jnp.float32, low / len(cuts), high / len(cuts))
        return jnp.repeat(jnp.exp(draws), shape[position] // blocks).reshape((-1,) + (1,) * (len(shape) - position - 1))

    factor_of = one(*cuts[0])
    for cut in cuts[1:]:
        factor_of = factor_of * one(*cut)
    return factor_of


def normal_values(key, dims, spread, reach, shards=(), kind=jnp.bfloat16):
    result = spread * jax.random.normal(key, dims, jnp.float32)
    if shards:
        result = result * block_scale(key, dims, shards, -0.22, 0.18)
    return jnp.clip(result, -reach, reach).astype(kind)


def setup_inputs(seed: int = 0, part: int = 0) -> dict:
    seeds = jax.random.split(jax.random.key(seed), 12)
    part_keys = jax.random.split(jax.random.fold_in(seeds[11], part), 12)
    return {
        "tokens": normal_values(part_keys[0], (TOKENS, D), 1.0, 6.0, ((0, 4),)),
        "norm_in": jnp.clip(1.0 + 0.18 * jax.random.normal(seeds[1], (D,), jnp.float32), 0.099609375, 1.8984375).astype(jnp.bfloat16),
        "w_value": normal_values(seeds[2], (D, D), D ** -0.5, 0.125, ((0, 4), (1, 4))),
        "w_gate": normal_values(seeds[3], (D, D), D ** -0.5, 0.125, ((0, 4), (1, 4))),
        "conv_kernel": draw_conv_kernel(jax.random.fold_in(seeds[11], 71), part),
        "ln_gain": jnp.clip(1.0 + 0.18 * jax.random.normal(seeds[5], (D,), jnp.float32), 0.099609375, 1.8984375).astype(jnp.bfloat16),
        "ln_shift": normal_values(seeds[6], (D,), 0.5, 3.0),
        "w_out": normal_values(seeds[7], (D, D), D ** -0.5, 0.125, ((0, 4), (1, 4))),
        "norm_mlp": jnp.clip(1.0 + 0.18 * jax.random.normal(seeds[8], (D,), jnp.float32), 0.099609375, 1.8984375).astype(jnp.bfloat16),
        "w_up": normal_values(seeds[9], (D, FF), D ** -0.5, 0.125, ((0, 4), (1, 4))),
        "w_down": normal_values(seeds[10], (FF, D), FF ** -0.5, 0.0625, ((0, 4), (1, 4))),
    }


def rms_scale(values, gain):
    as_float = values.astype(jnp.float32)
    scaled = as_float * lax.rsqrt(lax.optimization_barrier(jnp.mean(as_float * as_float, axis=-1, keepdims=True)) + 1e-06)
    return scaled * gain.astype(jnp.float32)

def grouped_sum(left, right, groups):
    inner = left.shape[1] // groups
    partials = jnp.einsum('stc,tcd->std', left.reshape(left.shape[0], groups, inner).astype(jnp.float32), right.reshape(groups, inner, right.shape[1]).astype(jnp.float32), precision=lax.Precision.HIGHEST)
    rounded = lax.optimization_barrier(partials.astype(jnp.bfloat16))
    return lax.optimization_barrier(jnp.sum(rounded.astype(jnp.float32), axis=1))

def reference(tokens, norm_in, w_value, w_gate, conv_kernel, ln_gain, ln_shift, w_out, norm_mlp, w_up, w_down):

    def one_sequence(sequence):
        normed_in = rms_scale(sequence, norm_in).astype(jnp.bfloat16)
        values_f = jnp.dot(normed_in, w_value, preferred_element_type=jnp.float32)
        gate_act = jnp.dot(normed_in, w_gate, preferred_element_type=jnp.float32)
        gated = values_f * jax.nn.sigmoid(gate_act)
        padded = jnp.pad(gated, ((KERNEL - 1, 0), (0, 0)))
        convolved = jnp.zeros_like(gated)
        for tap_index in range(KERNEL):
            convolved = convolved + conv_kernel[tap_index][None, :] * padded[tap_index:tap_index + SEQ]
        chan_mean = lax.optimization_barrier(jnp.mean(convolved, axis=-1, keepdims=True))
        chan_msq = lax.optimization_barrier(jnp.mean(convolved * convolved, axis=-1, keepdims=True))
        variance = chan_msq - chan_mean * chan_mean
        normed = (convolved - chan_mean) * lax.rsqrt(variance + 1e-05)
        normed = normed * ln_gain.astype(jnp.float32) + ln_shift.astype(jnp.float32)
        activated = jax.nn.silu(normed).astype(jnp.bfloat16)
        mixed = grouped_sum(activated, w_out, N_TP)
        residual = sequence.astype(jnp.float32) + mixed
        normed_mlp = rms_scale(residual, norm_mlp).astype(jnp.bfloat16)
        up_act = jnp.dot(normed_mlp, w_up, preferred_element_type=jnp.float32)
        hidden = jnp.square(jax.nn.relu(up_act)).astype(jnp.bfloat16)
        return (residual + grouped_sum(hidden, w_down, N_TP)).astype(jnp.bfloat16)
    sequences = tokens.reshape(N_FS, SEQ, D)
    return lax.map(one_sequence, sequences).reshape(TOKENS, D)
```

```python
import functools

import jax
import jax.numpy as jnp
from jax import lax
from jax.experimental import pallas as pl
from jax.experimental.pallas import tpu as pltpu
from jax.sharding import PartitionSpec as P

MESH = pl.DeviceIdType.MESH
PIECES = 4
PAD = 32


def rms_rows(x, gain):
    return x * lax.rsqrt(jnp.mean(x * x, axis=-1, keepdims=True) + 1e-06) * gain


def groups_of(n):
    return 2 if n >= 512 else 1


def kernel(
    F, T,
    tok_h, norm_in, conv_h, ln_gain, ln_shift, norm_mlp, wv, wg, wo, wu, wd,
    out,
    tok, conv_k, normed, gv, gg, go, gu, gd, gated, conv, act, part, pr, rs, resid, nm, hidden, fin, fpr, rs2,
    sum_e, ret, st_own, st_recv, nm_own,
    local_sem, zsend_r, zsend_l, zrecv_r, zrecv_l, ysend_r, ysend_l, yrecv_r, yrecv_l,
    rest_send, rest_recv, st_send, st_rsem, md_send, md_recv, mx_send, mx_recv,
    agd_send, agd_recv, agx_send, agx_recv, give_sem, fd_send, fd_recv, fx_send, fx_recv, ret_send, ret_recv,
):
    g = lax.axis_index("grp")
    z = lax.axis_index("fs")
    t = lax.axis_index("tp")
    S, D = tok.shape
    R, C = wv.shape
    H = wu.shape[1]
    N = wo.shape[1]
    taps = conv_k.shape[0]
    rows = S // T
    half = T // 2
    R2, C2, H2 = R // 2, C // 2, H // 2
    HB = H // PIECES
    G = groups_of(N)
    subs = PIECES // G
    GC, HC = N // G, H2 // subs
    other = 1 - g
    n_chunks = 3 + 2 * PIECES
    first_down = 3 + PIECES
    core = lax.rem(t, 2)
    chip = lax.div(t, 2)
    partner = t + 1 - 2 * core

    at_left, at_right = z == 0, z == F - 1
    is_end = jnp.logical_or(at_left, at_right)
    not_end = jnp.logical_not(is_end)
    help_left, help_right = z == 1, z == F - 2

    def upper(c):
        return int(c >= 3)

    def has_rest(c):
        return c >= 1

    def when_right(c):
        return pl.when(z < F - 1 - upper(c))

    def when_left(c):
        return pl.when(z > 0 + upper(c))

    def for_ends(body):
        @pl.when(at_left)
        def _():
            body(z + 1)

        @pl.when(at_right)
        def _():
            body(z - 1)

    def for_helpers(body):
        @pl.when(help_left)
        def _():
            body(z - 1)

        @pl.when(help_right)
        def _():
            body(z + 1)

    def for_middle(body):
        @pl.when(not_end)
        def _():
            body()

    def mult(i, k):
        return pl.multiple_of(i, k)

    def own(c, h):
        if c < 3:
            ref, size = ((wv, R2), (wg, R2), (wo, C2))[c]
            return ref.at[pl.ds(mult(h * size, size), size), :]
        if c < first_down:
            return wu.at[pl.ds(mult(h * R2, R2), R2), pl.ds((c - 3) * HB, HB)]
        q, r = divmod(c - first_down, subs)
        return wd.at[pl.ds(mult(h * H2 + r * HC, HC), HC), pl.ds(q * GC, GC)]

    def slot(c, src, h):
        if c < 2:
            return (gv, gg)[c].at[pl.ds(mult(src * R + h * R2, R2), R2), :]
        if c == 2:
            return go.at[src, pl.ds(mult(h * C2, C2), C2), :]
        if c < first_down:
            return gu.at[c - 3, pl.ds(mult(src * R + h * R2, R2), R2), :]
        q, r = divmod(c - first_down, subs)
        return gd.at[src, q, pl.ds(mult(h * H2 + r * HC, HC), HC), :]

    def remote(src_ref, dst_ref, send, recv, device):
        return pltpu.make_async_remote_copy(
            src_ref=src_ref, dst_ref=dst_ref, send_sem=send, recv_sem=recv,
            device_id=device, device_id_type=MESH,
        )

    loads = [
        pltpu.make_async_copy(tok_h, tok, local_sem.at[0]),
        pltpu.make_async_copy(conv_h, conv_k, local_sem.at[1]),
    ]
    for copy in loads:
        copy.start()

    peers = [lax.rem(t + i, T) for i in range(T)]
    barrier = pltpu.get_barrier_semaphore()

    def greet(device):
        pl.semaphore_signal(barrier, inc=1, device_id=device, device_id_type=MESH)

    greet((other, z, t))
    for i in range(1, T):
        greet((g, z, peers[i]))

    @pl.when(z > 0)
    def _():
        greet((g, z - 1, t))

    @pl.when(z < F - 1)
    def _():
        greet((g, z + 1, t))

    ends = lax.div(z + F - 1, F) + lax.div(2 * F - 2 - z, F)
    with jax.named_scope("bar"):
        pl.semaphore_wait(barrier, T + ends)

    ys, yr = (ysend_r, ysend_l), (yrecv_r, yrecv_l)

    def own_right(c):
        return remote(own(c, g), slot(c, z, g), zsend_r.at[c, 0], zrecv_r.at[c, 1], (g, z + 1, t))

    def own_left(c):
        return remote(own(c, g), slot(c, z, g), zsend_l.at[c, 0], zrecv_l.at[c, 1], (g, z - 1, t))

    def right_hop(c, d, src):
        return remote(slot(c, src, g), slot(c, src, g), zsend_r.at[c, d], zrecv_r.at[c, min(d + 1, F - 1)], (g, z + 1, t))

    def left_hop(c, d, src):
        return remote(slot(c, src, g), slot(c, src, g), zsend_l.at[c, d], zrecv_l.at[c, min(d + 1, F - 1)], (g, z - 1, t))

    def arrival(c, d, src, left):
        sems = zrecv_l if left else zrecv_r
        return remote(slot(c, src, g), slot(c, src, g), zsend_r.at[c, d], sems.at[c, d], (other, z, t))

    def across(c, d, src, left):
        return remote(slot(c, src, g), slot(c, src, g), ys[left].at[c, d], yr[left].at[c, d], (other, z, t))

    def across_arrival(c, d, src, left):
        return remote(slot(c, src, other), slot(c, src, other), ys[left].at[c, d], yr[left].at[c, d], (other, z, t))

    def own_rest(c, helper):
        return remote(own(c, other), slot(c, z, other), rest_send.at[c], rest_recv.at[c], (g, helper, t))

    def own_send(c, act_on):
        @when_right(c)
        def _():
            act_on(own_right(c))

        @when_left(c)
        def _():
            act_on(own_left(c))

    def start(copy):
        copy.start()

    def sent(copy):
        copy.wait_send()

    def mid(c):
        for_middle(lambda: own_send(c, start))

    def end(c, first=True, second=True):
        @pl.when(is_end)
        def _():
            if first:
                own_send(c, start)
            if second and has_rest(c):
                for_ends(lambda helper: own_rest(c, helper).start())

    def both(d, body, c=0):
        @pl.when(jnp.logical_and(z - d >= 0, z < F - upper(c)))
        def _():
            body(z - d, 0)

        @pl.when(jnp.logical_and(z + d < F, z >= 0 + upper(c)))
        def _():
            body(z + d, 1)

    def when_across(c, d, left):
        if d > 1 or not has_rest(c):
            return lambda body: body()
        return pl.when(z != (F - 2 if left else 1))

    def forward(c, d, src, left, act_on):
        if d < F - 1:
            if left:
                @when_left(c)
                def _():
                    act_on(left_hop(c, d, src))
            else:
                @when_right(c)
                def _():
                    act_on(right_hop(c, d, src))

        @when_across(c, d, left)
        def _():
            act_on(across(c, d, src, left))

    def service(c, *ds):
        for d in ds:
            with jax.named_scope(f"S{c}_{d}"):
                def body(src, left):
                    arrival(c, d, src, left).wait_recv()
                    forward(c, d, src, left, start)

                both(d, body, c)

    far = range(2, F)

    def y_wait(c, *ds):
        for d in ds:
            with jax.named_scope(f"Y{c}_{d}"):
                def body(src, left):
                    @when_across(c, d, left)
                    def _():
                        across_arrival(c, d, src, left).wait_recv()

                    if d == 1 and has_rest(c):
                        @pl.when(z == (F - 2 if left else 1))
                        def _():
                            remote(slot(c, src, other), slot(c, src, other), rest_send.at[c], rest_recv.at[c], (g, src, t)).wait_recv()

                both(d, body, c)

    def drain(c):
        own_send(c, sent)
        if has_rest(c):
            for_ends(lambda helper: own_rest(c, helper).wait_send())
        for d in range(1, F):
            both(d, lambda src, left: forward(c, d, src, left, sent), c)

    mid(0)
    end(0)
    copies = [
        pltpu.make_async_copy(wv, gv.at[pl.ds(mult(z * R, R), R), :], local_sem.at[2]),
        pltpu.make_async_copy(wg, gg.at[pl.ds(mult(z * R, R), R), :], local_sem.at[3]),
        pltpu.make_async_copy(wo, go.at[z], local_sem.at[4]),
    ]
    for j in range(PIECES):
        copies.append(
            pltpu.make_async_copy(
                wu.at[:, pl.ds(j * HB, HB)], gu.at[j, pl.ds(mult(z * R, R), R), :], local_sem.at[5 + j]
            )
        )
    for q in range(G):
        copies.append(pltpu.make_async_copy(wd.at[:, pl.ds(q * GC, GC)], gd.at[z, q], local_sem.at[5 + PIECES + q]))
    end(1)
    end(2)
    for copy in copies:
        copy.start()
    for copy in loads:
        copy.wait()

    block = 64

    def norm_step(i, carry):
        at = pl.ds(mult(i * block, block), block)
        x = tok[at, :].astype(jnp.float32)
        normed[at, :] = rms_rows(x, norm_in[...].reshape(1, D).astype(jnp.float32)).astype(jnp.bfloat16)
        return carry

    with jax.named_scope("norm"):
        lax.fori_loop(0, S // block, norm_step, 0)
    for copy in copies:
        copy.wait()

    service(0, 1)
    mid(1)
    service(0, *far)
    end(3)
    service(1, 1)
    mid(2)
    mid(3)
    service(1, *far)
    end(4)
    service(2, 1)
    y_wait(0, *range(1, F))
    y_wait(1, *range(1, F))

    tile = min(256, C)
    gated[0:PAD, :] = jnp.zeros((PAD, C), jnp.float32)

    def gate_step(i, carry):
        at = pl.ds(mult(i * tile, tile), tile)
        v = jnp.dot(normed[...], gv[:, at], preferred_element_type=jnp.float32)
        a = jnp.dot(normed[...], gg[:, at], preferred_element_type=jnp.float32)
        gated[PAD:, at] = v * jax.nn.sigmoid(a)
        return carry

    with jax.named_scope("gate"):
        lax.fori_loop(0, C // tile, gate_step, 0)

    span = 128
    lead = PAD - (taps - 1)

    def conv_step(i, carry):
        base = mult(i * span, span)
        first = jnp.zeros((span, 128), jnp.float32)
        second = jnp.zeros((span, 128), jnp.float32)
        for j in range(C // 128):
            lanes = pl.ds(j * 128, 128)
            window = gated[pl.ds(base, span + PAD), lanes]
            weights = conv_k[:, pl.ds(mult(t * C + j * 128, 128), 128)]
            acc = jnp.zeros((span, 128), jnp.float32)
            for k in range(taps):
                acc = acc + weights[k : k + 1, :] * window[lead + k : lead + k + span, :]
            conv[pl.ds(base, span), lanes] = acc
            first = first + acc
            second = second + acc * acc
        lane = lax.broadcasted_iota(jnp.int32, (span, 128), 1)
        both_sums = jnp.where(
            lane == 0,
            jnp.sum(first, axis=1, keepdims=True),
            jnp.where(lane == 1, jnp.sum(second, axis=1, keepdims=True), 0.0),
        )
        st_own[:, pl.ds(base, span)] = jnp.transpose(both_sums)[0:8, :]
        return carry

    spans = S // span
    with jax.named_scope("conv_a"):
        lax.fori_loop(0, spans // 2, conv_step, 0)
    service(3, 1)
    mid(4)
    with jax.named_scope("conv_b"):
        lax.fori_loop(spans // 2, spans, conv_step, 0)

    def stat_copy(i):
        return remote(st_own, st_recv.at[i], st_send.at[i], st_rsem.at[i], (g, z, peers[i]))

    for i in range(1, T):
        stat_copy(i).start()
    service(2, *far)
    end(5)
    service(4, 1)
    mid(5)
    for i in range(1, T):
        stat_copy(i).wait_recv()

    gain = ln_gain[pl.ds(mult(t * C, C), C)].reshape(1, C).astype(jnp.float32)
    shift = ln_shift[pl.ds(mult(t * C, C), C)].reshape(1, C).astype(jnp.float32)

    def act_step(i, carry):
        base = mult(i * span, span)
        at = pl.ds(base, span)
        sums = st_own[:, at]
        for k in range(1, T):
            sums = sums + st_recv[k, :, at]
        mean = sums[0:1, :] / D
        var = sums[1:2, :] / D - mean * mean
        scale = lax.rsqrt(var + 1e-05)
        mean_c = jnp.transpose(jnp.broadcast_to(mean, (128, span)))[:, 0:1]
        scale_c = jnp.transpose(jnp.broadcast_to(scale, (128, span)))[:, 0:1]
        n = (conv[at, :] - mean_c) * scale_c * gain + shift
        act[at, :] = (n * jax.nn.sigmoid(n)).astype(jnp.bfloat16)
        return carry

    with jax.named_scope("act"):
        lax.fori_loop(0, S // span, act_step, 0)
    y_wait(2, *range(1, F))

    def put_rows(ref, cols, value):
        for r in range(T):
            ref[r % 2, (r // 2) * rows : (r // 2 + 1) * rows, cols] = value[r * rows : (r + 1) * rows, :]

    def row_block(j):
        return pl.ds(mult(j * rows, rows), rows)

    def mirror(i):
        return lax.rem(chip + i, half)

    def mirror_source(i):
        return lax.rem(chip - i + half, half)

    def mix_pair(i):
        cols = pl.ds(mult(i * N, N), N)
        return remote(part.at[1 - core, :, cols], pr.at[:, cols], md_send.at[i], md_recv.at[i], (g, z, partner))

    def mix_copy(i, m):
        cols = pl.ds(mult(i * N, N), N)
        return remote(
            part.at[core, row_block(mirror(m)), cols], rs.at[m, :, cols], mx_send.at[i, m], mx_recv.at[i, m],
            (g, z, 2 * mirror(m) + core),
        )

    def out_step(i, carry):
        value = jnp.dot(act[...], go[i], preferred_element_type=jnp.float32).astype(jnp.bfloat16)
        put_rows(part, pl.ds(mult(i * N, N), N), value)
        mix_pair(i).start()
        return carry

    with jax.named_scope("outp"):
        lax.fori_loop(0, F, out_step, 0)

    def pair_step(i, carry):
        mix_pair(i).wait_recv()
        cols = pl.ds(mult(i * N, N), N)
        for m in range(1, half):
            at = row_block(mirror(m))
            pair = part[core, at, cols].astype(jnp.float32) + pr[at, cols].astype(jnp.float32)
            part[core, at, cols] = pair.astype(jnp.bfloat16)
            mix_copy(i, m).start()
        return carry

    with jax.named_scope("mixpair"):
        lax.fori_loop(0, F, pair_step, 0)
    service(3, *far)
    end(6)
    service(5, 1)
    mid(6)
    service(4, *far)

    def mix_wait(i, carry):
        for m in range(1, half):
            mix_copy(i, m).wait_recv()
        return carry

    with jax.named_scope("mixw"):
        lax.fori_loop(0, F, mix_wait, 0)

    small = 32

    def resid_step(i, carry):
        at = pl.ds(mult(i * small, small), small)
        mine = pl.ds(mult(t * rows + i * small, small), small)
        held = pl.ds(mult(chip * rows + i * small, small), small)
        total = part[core, held, :].astype(jnp.float32) + pr[held, :].astype(jnp.float32)
        for m in range(1, half):
            total = total + rs[m, at, :].astype(jnp.float32)
        r = tok[mine, :].astype(jnp.float32) + total
        resid[at, :] = r
        nm_own[at, :] = rms_rows(r, norm_mlp[...].reshape(1, D).astype(jnp.float32)).astype(jnp.bfloat16)
        return carry

    with jax.named_scope("resid"):
        lax.fori_loop(0, rows // small, resid_step, 0)
    mine = row_block(t)

    def give_copy(helper):
        return remote(nm_own, nm.at[1, mine, :], give_sem.at[0], give_sem.at[1], (g, helper, t))

    for_ends(lambda helper: give_copy(helper).start())
    for c in range(first_down, n_chunks):
        end(c, second=False)
    for c in range(first_down, n_chunks):
        end(c, first=False)

    def gather_x(w, i):
        src = nm_own if w == 0 else nm.at[w, mine, :]
        return remote(src, nm.at[w, mine, :], agx_send.at[w, i], agx_recv.at[w, i], (g, z, 2 * mirror(i) + core))

    def gather_x_arrival(w, i):
        there = row_block(2 * mirror_source(i) + core)
        return remote(nm.at[w, there, :], nm.at[w, there, :], agx_send.at[w, i], agx_recv.at[w, i], (g, z, partner))

    def gather_d(w, i):
        if i == 0:
            src = nm_own if w == 0 else nm.at[w, mine, :]
            return remote(src, nm.at[w, mine, :], agd_send.at[w, 0], agd_recv.at[w, 0], (g, z, partner))
        there = row_block(2 * mirror_source(i) + core)
        return remote(nm.at[w, there, :], nm.at[w, there, :], agd_send.at[w, i], agd_recv.at[w, i], (g, z, partner))

    def gather_d_arrival(w, i):
        there = row_block(2 * mirror_source(i) + 1 - core)
        return remote(nm.at[w, there, :], nm.at[w, there, :], agd_send.at[w, i], agd_recv.at[w, i], (g, z, partner))

    def gather_start(w):
        for i in range(1, half):
            gather_x(w, i).start()
        gather_d(w, 0).start()

    def gather_pass(w):
        for i in range(1, half):
            gather_x_arrival(w, i).wait_recv()
            gather_d(w, i).start()

    def gather_wait(w):
        for i in range(half):
            gather_d_arrival(w, i).wait_recv()

    def gather_first():
        gather_start(0)
        nm[0, mine, :] = nm_own[...]

    for_middle(gather_first)
    service(6, 1)
    mid(7)
    service(5, *far)
    with jax.named_scope("gpass0"):
        for_middle(lambda: gather_pass(0))
    service(7, 1)
    mid(8)
    with jax.named_scope("gwait0"):
        for_middle(lambda: gather_wait(0))

    utile = min(256, HB)

    def up_block(w, j):
        def up_step(i, carry):
            at = pl.ds(mult(i * utile, utile), utile)
            a = jnp.dot(nm[w], gu[j, :, at], preferred_element_type=jnp.float32)
            a = jnp.maximum(a, 0.0)
            hidden[w, :, pl.ds(mult(j * HB + i * utile, utile), utile)] = (a * a).astype(jnp.bfloat16)
            return carry

        lax.fori_loop(0, HB // utile, up_step, 0)

    def up(j):
        y_wait(3 + j, *range(1, F))
        with jax.named_scope(f"up{j}"):
            for_middle(lambda: up_block(0, j))

    up(0)
    up(1)
    service(6, *far)
    up(2)
    service(8, 1)
    mid(9)
    up(3)

    def columns(q):
        return pl.ds(q * GC, GC)

    def fin_pair(w, q, src):
        return remote(
            fin.at[w, src, 1 - core, :, columns(q)], fpr.at[w, src, :, columns(q)],
            fd_send.at[w * F + src, q], fd_recv.at[w * F + src, q], (g, z, partner),
        )

    def fin_copy(w, q, src, m):
        return remote(
            fin.at[w, src, core, row_block(mirror(m)), columns(q)], rs2.at[w, src, m, :, columns(q)],
            fx_send.at[w * F + src, q * half + m], fx_recv.at[w * F + src, q * half + m],
            (g, z, 2 * mirror(m) + core),
        )

    def ret_copy(q, src, device):
        return remote(
            sum_e.at[src, :, columns(q)], ret.at[src, :, columns(q)], ret_send.at[src, q], ret_recv.at[src, q],
            (g, device, t),
        )

    def units(w, d, body):
        def run(*_):
            if d == 0:
                body(z)
                return

            def step(s, carry):
                body(z + (2 * s - 1) * d)
                return carry

            lax.fori_loop(1 - lax.div(z + F - d, F), 1 + lax.div(2 * F - 1 - z - d, F), step, 0)

        (for_helpers if w else for_middle)(run)

    def down(w, q, *ds):
        def body(src):
            value = jnp.dot(hidden[w], gd[src, q], preferred_element_type=jnp.float32).astype(jnp.bfloat16)
            put_rows(fin.at[w, src], columns(q), value)
            fin_pair(w, q, src).start()

        for d in ds:
            with jax.named_scope(f"down{w}{q}{d}"):
                units(w, d, body)

    def pair(w, q, *ds):
        def body(src):
            fin_pair(w, q, src).wait_recv()
            for m in range(1, half):
                at = row_block(mirror(m))
                total = fin[w, src, core, at, columns(q)].astype(jnp.float32) + fpr[w, src, at, columns(q)].astype(jnp.float32)
                fin[w, src, core, at, columns(q)] = total.astype(jnp.bfloat16)
                fin_copy(w, q, src, m).start()

        for d in ds:
            with jax.named_scope(f"pair{w}{q}{d}"):
                units(w, d, body)

    def finish(w, q, *ds):
        def body(src):
            for m in range(1, half):
                fin_copy(w, q, src, m).wait_recv()
            at = row_block(chip)
            total = fin[w, src, core, at, columns(q)].astype(jnp.float32) + fpr[w, src, at, columns(q)].astype(jnp.float32)
            for m in range(1, half):
                total = total + rs2[w, src, m, :, columns(q)].astype(jnp.float32)
            if w == 0:
                cols = pl.ds(mult(src * N + q * GC, GC), GC)
                out[:, cols] = (resid[:, cols] + total).astype(jnp.bfloat16)
            else:
                sum_e[src, :, columns(q)] = total.astype(jnp.bfloat16)
                for_helpers(lambda device: ret_copy(q, src, device).start())

        for d in ds:
            with jax.named_scope(f"fin{w}{q}{d}"):
                units(w, d, body)

    first_cols, last_cols = range(G - 1), G - 1

    for q in range(G):
        down(0, q, 0)

    def share(device):
        remote(nm_own, nm.at[1, mine, :], give_sem.at[0], give_sem.at[1], (g, device, t)).wait_recv()
        gather_start(1)

    with jax.named_scope("share"):
        for_helpers(share)
    service(7, *far)
    for q in range(G):
        pair(0, q, 0)
    service(9, 1)
    mid(10)
    service(8, *far)
    with jax.named_scope("gpass1"):
        for_helpers(lambda device: gather_pass(1))
    for c in range(first_down, first_down + subs * (G - 1)):
        y_wait(c, 1)
    for q in first_cols:
        down(0, q, 1)
    with jax.named_scope("gwait1"):
        for_helpers(lambda device: gather_wait(1))

    def up_end(lo, hi):
        def body(device):
            def step(j, carry):
                up_block(1, j)
                return carry

            lax.fori_loop(lo, hi, step, 0)

        with jax.named_scope("up_end"):
            for_helpers(body)

    up_end(0, PIECES // 2)
    service(10, 1)
    up_end(PIECES // 2, PIECES)
    service(9, *far)
    for q in first_cols:
        pair(0, q, 1)
    for q in range(G):
        down(1, q, 0)
    for q in first_cols:
        down(1, q, 1)
    for c in range(first_down, first_down + subs * (G - 1)):
        y_wait(c, *far)
    service(10, *far)
    for q in first_cols:
        down(0, q, *far)
        down(1, q, *far)
    for q in range(G):
        pair(1, q, 0)
    for q in first_cols:
        pair(1, q, 1)
        pair(0, q, *far)
        pair(1, q, *far)
    late = range(first_down + subs * (G - 1), n_chunks)
    for c in late:
        y_wait(c, 1)
    down(0, last_cols, 1)
    down(1, last_cols, 1)
    for c in range(first_down):
        drain(c)
    pair(0, last_cols, 1)
    pair(1, last_cols, 1)
    for q in range(G):
        finish(1, q, 0)
        finish(0, q, 0)
    for q in first_cols:
        finish(1, q, 1, *far)
        finish(0, q, 1, *far)
    for c in late:
        y_wait(c, *far)
    down(1, last_cols, *far)
    down(0, last_cols, *far)
    pair(1, last_cols, *far)
    pair(0, last_cols, *far)
    finish(1, last_cols, 1)
    finish(0, last_cols, 1)
    for c in range(first_down, n_chunks):
        drain(c)
    finish(1, last_cols, *far)
    finish(0, last_cols, *far)

    def take(helper):
        for q in range(G):
            def step(src, carry):
                ret_copy(q, src, helper).wait_recv()
                cols = pl.ds(mult(src * N + q * GC, GC), GC)
                out[:, cols] = (resid[:, cols] + ret[src, :, columns(q)].astype(jnp.float32)).astype(jnp.bfloat16)
                return carry

            lax.fori_loop(0, F, step, 0)

    with jax.named_scope("take"):
        for_ends(take)

    for_ends(lambda helper: give_copy(helper).wait_send())
    for i in range(1, T):
        stat_copy(i).wait_send()

    def drain_mix(i, carry):
        mix_pair(i).wait_send()
        for m in range(1, half):
            mix_copy(i, m).wait_send()
        return carry

    lax.fori_loop(0, F, drain_mix, 0)

    def drain_layer(w):
        for i in range(1, half):
            gather_x(w, i).wait_send()
        for i in range(half):
            gather_d(w, i).wait_send()

        def step(src, carry):
            for q in range(G):
                fin_pair(w, q, src).wait_send()
                for m in range(1, half):
                    fin_copy(w, q, src, m).wait_send()
                if w:
                    for_helpers(lambda device: ret_copy(q, src, device).wait_send())
            return carry

        lax.fori_loop(0, F, step, 0)

    for_middle(lambda: drain_layer(0))
    for_helpers(lambda device: drain_layer(1))


def solution(mesh):
    F, T = mesh.shape["fs"], mesh.shape["tp"]

    def step(tokens, norm_in, w_value, w_gate, conv_kernel, ln_gain, ln_shift, w_out, norm_mlp, w_up, w_down):
        S, D = tokens.shape
        R, C = w_value.shape
        H = w_up.shape[1]
        N = w_out.shape[1]
        rows, half, G = S // T, T // 2, groups_of(N)
        chunks = 3 + 2 * PIECES
        bf16, f32 = jnp.bfloat16, jnp.float32
        dma = pltpu.SemaphoreType.DMA
        vmem = pl.BlockSpec(memory_space=pltpu.VMEM)
        anywhere = pl.BlockSpec(memory_space=pl.ANY)
        return pl.pallas_call(
            functools.partial(kernel, F, T),
            out_shape=jax.ShapeDtypeStruct((rows, D), bf16),
            in_specs=[anywhere, vmem, anywhere, vmem, vmem, vmem] + [anywhere] * 5,
            out_specs=vmem,
            scratch_shapes=[
                pltpu.VMEM((S, D), bf16),
                pltpu.VMEM(conv_kernel.shape, f32),
                pltpu.VMEM((S, D), bf16),
                pltpu.VMEM((D, C), bf16),
                pltpu.VMEM((D, C), bf16),
                pltpu.VMEM((F, C, N), bf16),
                pltpu.VMEM((PIECES, D, H // PIECES), bf16),
                pltpu.VMEM((F, G, H, N // G), bf16),
                pltpu.VMEM((S + PAD, C), f32),
                pltpu.VMEM((S, C), f32),
                pltpu.VMEM((S, C), bf16),
                pltpu.VMEM((2, half * rows, D), bf16),
                pltpu.VMEM((half * rows, D), bf16),
                pltpu.VMEM((half, rows, D), bf16),
                pltpu.VMEM((rows, D), f32),
                pltpu.VMEM((2, S, D), bf16),
                pltpu.VMEM((2, S, H), bf16),
                pltpu.VMEM((2, F, 2, half * rows, N), bf16),
                pltpu.VMEM((2, F, half * rows, N), bf16),
                pltpu.VMEM((2, F, half, rows, N), bf16),
                pltpu.VMEM((F, rows, N), bf16),
                pltpu.VMEM((F, rows, N), bf16),
                pltpu.VMEM((8, S), f32),
                pltpu.VMEM((T, 8, S), f32),
                pltpu.VMEM((rows, D), bf16),
                dma((5 + PIECES + G,)),
            ]
            + [dma((chunks, F))] * 8
            + [dma((chunks,))] * 2
            + [dma((T,))] * 2
            + [dma((F,))] * 2
            + [dma((F, half))] * 2
            + [dma((2, half))] * 4
            + [dma((2,))]
            + [dma((2 * F, G))] * 2
            + [dma((2 * F, G * half))] * 2
            + [dma((F, G))] * 2,
            compiler_params=pltpu.CompilerParams(
                collective_id=0, has_side_effects=True, vmem_limit_bytes=62 * 1024 * 1024
            ),
        )(
            tokens, norm_in, conv_kernel, ln_gain, ln_shift, norm_mlp, w_value, w_gate, w_out, w_up, w_down,
        )

    in_specs = (
        P(("grp", "fs"), None), P(), P("fs", "tp"), P("fs", "tp"), P(), P(), P(),
        P("tp", "fs"), P(), P("fs", "tp"), P("tp", "fs"),
    )
    return jax.shard_map(
        step, mesh=mesh, in_specs=in_specs, out_specs=P(("grp", "fs", "tp"), None), check_vma=False
    )
```

```python
import functools

import jax
import jax.numpy as jnp
from jax import lax
from jax.experimental import pallas as pl
from jax.experimental.pallas import tpu as pltpu
from jax.sharding import PartitionSpec as P

MESH = pl.DeviceIdType.MESH
PIECES = 4
PAD = 32
RING = 6


def rms_rows(x, gain):
    return x * lax.rsqrt(jnp.mean(x * x, axis=-1, keepdims=True) + 1e-06) * gain


def groups_of(n):
    return 2 if n >= 512 else 1


def kernel(
    F, T,
    tok_h, norm_in, conv_h, ln_gain, ln_shift, norm_mlp, wv, wg, wo, wu, wd,
    out,
    tok, conv_k, normed, gv, gg, go, gu, gd, gated, conv, act, part, pr, rs, resid, nm, hidden, fin, fpr, rs2,
    ret, st_own, st_recv, nm_own,
    local_sem, own_sem, rest_sem, zsend, zrecv, ysend, yrecv, yrecv_all, st_send, st_rsem, md_send, md_recv, mx_send, mx_recv,
    agd_send, agd_recv, agx_send, agx_recv, give_sem, fd_send, fd_recv, fx_send, fx_recv, ret_send, ret_recv,
):
    g = lax.axis_index("grp")
    z = lax.axis_index("fs")
    t = lax.axis_index("tp")
    S, D = tok.shape
    R, C = wv.shape
    H = wu.shape[1]
    N = wo.shape[1]
    taps = conv_k.shape[0]
    rows = S // T
    half = T // 2
    R2, R4, C2, H2 = R // 2, R // 4, C // 2, H // 2
    HB = H // PIECES
    G = groups_of(N)
    subs = PIECES // G
    GC, HC = N // G, H2 // subs
    other = 1 - g
    n_chunks = 3 + 2 * PIECES
    first_down = 3 + PIECES
    early = range(first_down, first_down + subs * (G - 1))
    late = range(first_down + subs * (G - 1), n_chunks)
    second = n_chunks
    core = lax.rem(t, 2)
    chip = lax.div(t, 2)
    partner = t + 1 - 2 * core

    at_left, at_right = z == 0, z == F - 1
    is_end = jnp.logical_or(at_left, at_right)
    not_end = jnp.logical_not(is_end)
    help_left, help_right = z == 1, z == F - 2

    def upper(c):
        return int(3 <= c < n_chunks)

    def has_rest(c):
        return c >= 1

    def when_right(c):
        return pl.when(z < F - 1 - upper(c))

    def when_left(c):
        return pl.when(z > 0 + upper(c))

    def for_ends(body):
        @pl.when(at_left)
        def _():
            body(z + 1, 0)

        @pl.when(at_right)
        def _():
            body(z - 1, 1)

    def for_helpers(body):
        @pl.when(help_left)
        def _():
            body(z - 1)

        @pl.when(help_right)
        def _():
            body(z + 1)

    def for_middle(body):
        @pl.when(not_end)
        def _():
            body()

    def mult(i, k):
        return pl.multiple_of(i, k)

    def own(c, h):
        if c in (0, second):
            return wv.at[pl.ds(mult(h * R2 + (R4 if c else 0), R4), R4), :]
        if c < 3:
            ref, size = ((wv, R2), (wg, R2), (wo, C2))[c]
            return ref.at[pl.ds(mult(h * size, size), size), :]
        if c < first_down:
            return wu.at[pl.ds(mult(h * R2, R2), R2), pl.ds((c - 3) * HB, HB)]
        q, r = divmod(c - first_down, subs)
        return wd.at[pl.ds(mult(h * H2 + r * HC, HC), HC), pl.ds(q * GC, GC)]

    def slot(c, src, h):
        if c in (0, second):
            return gv.at[pl.ds(mult(src * R + h * R2 + (R4 if c else 0), R4), R4), :]
        if c < 2:
            return gg.at[pl.ds(mult(src * R + h * R2, R2), R2), :]
        if c == 2:
            return go.at[src, pl.ds(mult(h * C2, C2), C2), :]
        if c < first_down:
            return gu.at[c - 3, pl.ds(mult(src * R + h * R2, R2), R2), :]
        q, r = divmod(c - first_down, subs)
        return gd.at[src, q, pl.ds(mult(h * H2 + r * HC, HC), HC), :]

    def remote(src_ref, dst_ref, send, recv, device):
        return pltpu.make_async_remote_copy(
            src_ref=src_ref, dst_ref=dst_ref, send_sem=send, recv_sem=recv,
            device_id=device, device_id_type=MESH,
        )

    loads = [
        pltpu.make_async_copy(tok_h, tok, local_sem.at[0]),
        pltpu.make_async_copy(conv_h, conv_k, local_sem.at[1]),
    ]
    for copy in loads:
        copy.start()

    peers = [lax.rem(t + i, T) for i in range(T)]
    barrier = pltpu.get_barrier_semaphore()

    def greet(device):
        pl.semaphore_signal(barrier, inc=1, device_id=device, device_id_type=MESH)

    greet((other, z, t))
    for i in range(1, T):
        greet((g, z, peers[i]))

    @pl.when(z > 0)
    def _():
        greet((g, z - 1, t))

    @pl.when(z < F - 1)
    def _():
        greet((g, z + 1, t))

    ends = lax.div(z + F - 1, F) + lax.div(2 * F - 2 - z, F)
    def greet_mirrors(there):
        for m in range(1, half):
            greet((g, there, 2 * lax.rem(chip + m, half) + core))

    for_ends(lambda helper, left: greet_mirrors(helper))
    for_helpers(greet_mirrors)
    outer = lax.div(F + 1 - z, F) + lax.div(z + 2, F)
    with jax.named_scope("bar"):
        pl.semaphore_wait(barrier, T + ends + (half - 1) * outer)

    def index(d, left):
        return d - 1 if left else F - 1 - d

    order = (0, second, *range(1, n_chunks))

    def ring(c):
        return order.index(c) % RING

    def before(c):
        place = order.index(c) - RING
        return order[place] if place >= 0 else None

    def y_arrival(c, d, left):
        if c in early or c in late:
            return yrecv.at[c - first_down, index(d, left)]
        return yrecv_all.at[order.index(c)]

    def own_right(c):
        return remote(own(c, g), slot(c, z, g), own_sem.at[ring(c), 0], zrecv.at[c, index(1, 0)], (g, z + 1, t))

    def own_left(c):
        return remote(own(c, g), slot(c, z, g), own_sem.at[ring(c), 1], zrecv.at[c, index(1, 1)], (g, z - 1, t))

    def hop(c, d, src, left):
        here = slot(c, src, g)
        return remote(
            here, here, zsend.at[ring(c), index(d, left)], zrecv.at[c, index(d + 1, left)], (g, z - 1 if left else z + 1, t)
        )

    def arrival(c, d, src, left):
        here = slot(c, src, g)
        return remote(here, here, zsend.at[ring(c), index(d, left)], zrecv.at[c, index(d, left)], (other, z, t))

    def across(c, d, src, left, h=g):
        here = slot(c, src, h)
        return remote(here, here, ysend.at[ring(c), index(d, left)], y_arrival(c, d, left), (other, z, t))

    def own_rest(c, helper, left):
        return remote(own(c, other), slot(c, z, other), rest_sem.at[ring(c)], y_arrival(c, 1, left), (g, helper, t))

    low = z < F // 2
    high = jnp.logical_not(low)
    upside = lax.div(z, F // 2)

    def on_side(cond, left, side):
        if side is None:
            return cond
        return jnp.logical_and(cond, high if bool(left) == (side == "near") else low)

    def own_send(c, act_on, side=None):
        @pl.when(on_side(z < F - 1 - upper(c), 1, side))
        def _():
            act_on(own_right(c))

        @pl.when(on_side(z > 0 + upper(c), 0, side))
        def _():
            act_on(own_left(c))

    def start(copy):
        copy.start()

    def sent(copy):
        copy.wait_send()

    def mid(c, side=None):
        if before(c) is not None:
            for_middle(lambda: own_send(before(c), sent, side))
        for_middle(lambda: own_send(c, start, side))

    def rest_send(c, act_on):
        if has_rest(c):
            for_ends(lambda helper, left: act_on(own_rest(c, helper, left)))

    def end(c, first=True, rest=True):
        @pl.when(is_end)
        def _():
            if first:
                if before(c) is not None:
                    own_send(before(c), sent)
                own_send(c, start)
            if rest:
                if before(c) is not None:
                    rest_send(before(c), sent)
                rest_send(c, start)

    def both(d, body, c=0, side=None, who=None):
        def cond(base, left):
            base = on_side(base, left, side)
            return base if who is None else jnp.logical_and(base, is_end if who == "ends" else not_end)

        @pl.when(cond(jnp.logical_and(z - d >= 0, z < F - upper(c)), 0))
        def _():
            body(z - d, 0)

        @pl.when(cond(jnp.logical_and(z + d < F, z >= 0 + upper(c)), 1))
        def _():
            body(z + d, 1)

    def when_across(c, d, left):
        if d > 1 or not has_rest(c):
            return lambda body: body()
        return pl.when(z != (F - 2 if left else 1))

    def forward(c, d, src, left, act_on):
        if d < F - 1:
            @(when_left if left else when_right)(c)
            def _():
                act_on(hop(c, d, src, left))

        @when_across(c, d, left)
        def _():
            act_on(across(c, d, src, left))

    def service(c, *ds, side=None, who=None):
        for d in ds:
            with jax.named_scope(f"S{c}_{d}{side or ''}"):
                def body(src, left):
                    arrival(c, d, src, left).wait_recv()
                    forward(c, d, src, left, start)

                if before(c) is not None:
                    both(d, lambda src, left: forward(before(c), d, src, left, sent), before(c), side, who)
                both(d, body, c, side, who)

    every, far = range(1, F), range(2, F)

    def y_wait(c, *ds, side=None):
        for d in ds:
            with jax.named_scope(f"Y{c}_{d}{side or ''}"):
                def body(src, left):
                    across(c, d, src, left, other).wait_recv()

                both(d, body, c, side)

    def y_wait_all(c):
        if c in (0, second):
            got = gv.at[0 : (F - 1) * R4, :]
        elif c < 3:
            got = gg.at[0 : (F - 1) * R2, :] if c == 1 else go.at[0 : F - 1, 0:C2, :]
        else:
            got = gu.at[c - 3, 0 : (F - 1) * R2, :]

        def body():
            remote(got, got, yrecv_all.at[order.index(c)], yrecv_all.at[order.index(c)], (other, z, t)).wait_recv()

        with jax.named_scope(f"Y{c}"):
            for_middle(body) if upper(c) else body()

    def drain(c):
        own_send(c, sent)
        rest_send(c, sent)
        for d in range(1, F):
            both(d, lambda src, left: forward(c, d, src, left, sent), c)

    for c in (0, second):
        mid(c)
        end(c, rest=False)
    mid(1, "near")
    end(1, rest=False)
    end(2, rest=False)
    copies = [
        pltpu.make_async_copy(wv, gv.at[pl.ds(mult(z * R, R), R), :], local_sem.at[2]),
        pltpu.make_async_copy(wg, gg.at[pl.ds(mult(z * R, R), R), :], local_sem.at[3]),
        pltpu.make_async_copy(wo, go.at[z], local_sem.at[4]),
    ]
    for j in range(PIECES):
        copies.append(
            pltpu.make_async_copy(
                wu.at[:, pl.ds(j * HB, HB)], gu.at[j, pl.ds(mult(z * R, R), R), :], local_sem.at[5 + j]
            )
        )
    for q in range(G):
        copies.append(pltpu.make_async_copy(wd.at[:, pl.ds(q * GC, GC)], gd.at[z, q], local_sem.at[5 + PIECES + q]))
    end(second, first=False)
    end(1, first=False)
    end(2, first=False)
    end(3)
    for copy in copies:
        copy.start()
    for copy in loads:
        copy.wait()

    block = 64

    def norm_step(i, carry):
        at = pl.ds(mult(i * block, block), block)
        x = tok[at, :].astype(jnp.float32)
        normed[at, :] = rms_rows(x, norm_in[...].reshape(1, D).astype(jnp.float32)).astype(jnp.bfloat16)
        return carry

    with jax.named_scope("norm"):
        lax.fori_loop(0, S // block, norm_step, 0)
    for copy in copies:
        copy.wait()

    service(0, 1)
    service(second, 1)
    mid(1, "far")
    service(1, 1, side="near")
    mid(2, "far")
    service(1, 1, who="ends")
    service(0, *far)
    service(second, *far)
    end(4)
    service(1, 1, side="far", who="middle")
    service(2, 1, side="near")
    mid(3)
    mid(4)
    service(1, *far)
    mid(2, "near")
    end(5)
    service(2, 1, side="far")
    y_wait_all(0)
    y_wait_all(second)
    y_wait_all(1)

    tile = min(256, C)
    gated[0:PAD, :] = jnp.zeros((PAD, C), jnp.float32)

    def gate_step(i, carry):
        at = pl.ds(mult(i * tile, tile), tile)
        v = jnp.dot(normed[...], gv[:, at], preferred_element_type=jnp.float32)
        a = jnp.dot(normed[...], gg[:, at], preferred_element_type=jnp.float32)
        gated[PAD:, at] = v * jax.nn.sigmoid(a)
        return carry

    with jax.named_scope("gate"):
        lax.fori_loop(0, C // tile, gate_step, 0)

    span = 128
    lead = PAD - (taps - 1)

    def conv_step(i, carry):
        base = mult(i * span, span)
        first = jnp.zeros((span, 128), jnp.float32)
        second = jnp.zeros((span, 128), jnp.float32)
        for j in range(C // 128):
            lanes = pl.ds(j * 128, 128)
            window = gated[pl.ds(base, span + PAD), lanes]
            weights = conv_k[:, pl.ds(mult(t * C + j * 128, 128), 128)]
            acc = jnp.zeros((span, 128), jnp.float32)
            for k in range(taps):
                acc = acc + weights[k : k + 1, :] * window[lead + k : lead + k + span, :]
            conv[pl.ds(base, span), lanes] = acc
            first = first + acc
            second = second + acc * acc
        lane = lax.broadcasted_iota(jnp.int32, (span, 128), 1)
        both_sums = jnp.where(
            lane == 0,
            jnp.sum(first, axis=1, keepdims=True),
            jnp.where(lane == 1, jnp.sum(second, axis=1, keepdims=True), 0.0),
        )
        st_own[:, pl.ds(base, span)] = jnp.transpose(both_sums)[0:8, :]
        return carry

    spans = S // span
    end(6)
    service(2, *far, who="middle")
    with jax.named_scope("conv_a"):
        lax.fori_loop(0, spans // 2, conv_step, 0)
    service(3, 1, side="near")
    mid(5)
    service(3, 1, side="far")
    with jax.named_scope("conv_b"):
        lax.fori_loop(spans // 2, spans, conv_step, 0)

    def stat_copy(i):
        return remote(st_own, st_recv.at[i], st_send.at[0], st_rsem.at[i], (g, z, peers[i]))

    for i in range(1, T):
        stat_copy(i).start()
    end(7, rest=False)
    service(2, *far, who="ends")
    service(4, 1, side="far")
    service(4, 1, side="near")
    mid(6)
    for i in range(1, T):
        stat_copy(i).wait_recv()

    gain = ln_gain[pl.ds(mult(t * C, C), C)].reshape(1, C).astype(jnp.float32)
    shift = ln_shift[pl.ds(mult(t * C, C), C)].reshape(1, C).astype(jnp.float32)

    def act_step(i, carry):
        base = mult(i * span, span)
        at = pl.ds(base, span)
        sums = st_own[:, at]
        for k in range(1, T):
            sums = sums + st_recv[k, :, at]
        mean = sums[0:1, :] / D
        var = sums[1:2, :] / D - mean * mean
        scale = lax.rsqrt(var + 1e-05)
        mean_c = jnp.transpose(jnp.broadcast_to(mean, (128, span)))[:, 0:1]
        scale_c = jnp.transpose(jnp.broadcast_to(scale, (128, span)))[:, 0:1]
        n = (conv[at, :] - mean_c) * scale_c * gain + shift
        act[at, :] = (n * jax.nn.sigmoid(n)).astype(jnp.bfloat16)
        return carry

    with jax.named_scope("act"):
        lax.fori_loop(0, S // span, act_step, 0)
    y_wait_all(2)

    def put_rows(ref, cols, value):
        for r in range(T):
            ref[r % 2, (r // 2) * rows : (r // 2 + 1) * rows, cols] = value[r * rows : (r + 1) * rows, :]

    def row_block(j):
        return pl.ds(mult(j * rows, rows), rows)

    def mirror(i):
        return lax.rem(chip + i, half)

    def mirror_source(i):
        return lax.rem(chip - i + half, half)

    def mix_pair(i):
        cols = pl.ds(mult(i * N, N), N)
        return remote(part.at[1 - core, :, cols], pr.at[:, cols], md_send.at[0], md_recv.at[i], (g, z, partner))

    def mix_copy(i, m):
        cols = pl.ds(mult(i * N, N), N)
        return remote(
            part.at[core, row_block(mirror(m)), cols], rs.at[m, :, cols], mx_send.at[0], mx_recv.at[i, m - 1],
            (g, z, 2 * mirror(m) + core),
        )

    def out_step(i, carry):
        value = jnp.dot(act[...], go[i], preferred_element_type=jnp.float32).astype(jnp.bfloat16)
        put_rows(part, pl.ds(mult(i * N, N), N), value)
        mix_pair(i).start()
        return carry

    with jax.named_scope("outp"):
        lax.fori_loop(0, F, out_step, 0)

    def pair_step(i, carry):
        mix_pair(i).wait_recv()
        cols = pl.ds(mult(i * N, N), N)
        for m in range(1, half):
            at = row_block(mirror(m))
            pair = part[core, at, cols].astype(jnp.float32) + pr[at, cols].astype(jnp.float32)
            part[core, at, cols] = pair.astype(jnp.bfloat16)
            mix_copy(i, m).start()
        return carry

    with jax.named_scope("mixpair"):
        lax.fori_loop(0, F, pair_step, 0)
    service(3, *far)
    service(5, 1, side="far")
    service(5, 1, side="near")
    mid(7)

    def mix_wait(i, carry):
        for m in range(1, half):
            mix_copy(i, m).wait_recv()
        return carry

    with jax.named_scope("mixw"):
        lax.fori_loop(0, F, mix_wait, 0)

    small = 32

    def resid_step(i, carry):
        at = pl.ds(mult(i * small, small), small)
        mine = pl.ds(mult(t * rows + i * small, small), small)
        held = pl.ds(mult(chip * rows + i * small, small), small)
        total = part[core, held, :].astype(jnp.float32) + pr[held, :].astype(jnp.float32)
        for m in range(1, half):
            total = total + rs[m, at, :].astype(jnp.float32)
        r = tok[mine, :].astype(jnp.float32) + total
        resid[at, :] = r
        nm_own[at, :] = rms_rows(r, norm_mlp[...].reshape(1, D).astype(jnp.float32)).astype(jnp.bfloat16)
        return carry

    with jax.named_scope("resid"):
        lax.fori_loop(0, rows // small, resid_step, 0)
    mine = row_block(t)

    def give_copy(helper):
        return remote(nm_own, nm.at[1, mine, :], give_sem.at[0], give_sem.at[1], (g, helper, t))

    for_ends(lambda helper, left: give_copy(helper).start())
    end(8, rest=False)
    end(9, rest=False)
    end(7, first=False)
    end(10, rest=False)
    for c in range(8, n_chunks):
        end(c, first=False)

    def gather_x(w, i):
        src = nm_own if w == 0 else nm.at[w, mine, :]
        return remote(src, nm.at[w, mine, :], agx_send.at[w], agx_recv.at[w, i - 1], (g, z, 2 * mirror(i) + core))

    def gather_x_arrival(w, i):
        there = row_block(2 * mirror_source(i) + core)
        return remote(nm.at[w, there, :], nm.at[w, there, :], agx_send.at[w], agx_recv.at[w, i - 1], (g, z, partner))

    def gather_d(w, i):
        if i == 0:
            src = nm_own if w == 0 else nm.at[w, mine, :]
            return remote(src, nm.at[w, mine, :], agd_send.at[w], agd_recv.at[w, 0], (g, z, partner))
        there = row_block(2 * mirror_source(i) + core)
        return remote(nm.at[w, there, :], nm.at[w, there, :], agd_send.at[w], agd_recv.at[w, i], (g, z, partner))

    def gather_d_arrival(w, i):
        there = row_block(2 * mirror_source(i) + 1 - core)
        return remote(nm.at[w, there, :], nm.at[w, there, :], agd_send.at[w], agd_recv.at[w, i], (g, z, partner))

    def gather_start(w):
        for i in range(1, half):
            gather_x(w, i).start()
        gather_d(w, 0).start()

    def gather_pass(w):
        for i in range(1, half):
            gather_x_arrival(w, i).wait_recv()
            gather_d(w, i).start()

    def gather_wait(w):
        for i in range(half):
            gather_d_arrival(w, i).wait_recv()

    def gather_first():
        gather_start(0)
        nm[0, mine, :] = nm_own[...]

    for_middle(gather_first)
    service(4, *far)
    service(6, 1, side="far")
    service(6, 1, side="near")
    mid(8)
    service(5, *far)
    with jax.named_scope("gpass0"):
        for_middle(lambda: gather_pass(0))
    service(7, 1, side="far")
    service(7, 1, side="near")
    mid(9)
    with jax.named_scope("gwait0"):
        for_middle(lambda: gather_wait(0))

    utile = min(256, HB)

    def up_block(w, j):
        def up_step(i, carry):
            at = pl.ds(mult(i * utile, utile), utile)
            a = jnp.dot(nm[w], gu[j, :, at], preferred_element_type=jnp.float32)
            a = jnp.maximum(a, 0.0)
            hidden[w, :, pl.ds(mult(j * HB + i * utile, utile), utile)] = (a * a).astype(jnp.bfloat16)
            return carry

        lax.fori_loop(0, HB // utile, up_step, 0)

    def up(j):
        y_wait_all(3 + j)
        with jax.named_scope(f"up{j}"):
            for_middle(lambda: up_block(0, j))

    up(0)
    up(1)
    service(6, *far)
    up(2)

    def share(device):
        remote(nm_own, nm.at[1, mine, :], give_sem.at[0], give_sem.at[1], (g, device, t)).wait_recv()
        gather_start(1)

    with jax.named_scope("share"):
        for_helpers(share)
    service(8, 1, side="far")
    up(3)

    def columns(q):
        return pl.ds(q * GC, GC)

    def fin_pair(w, q, src):
        return remote(
            fin.at[w, src, 1 - core, :, columns(q)], fpr.at[w, src, :, columns(q)],
            fd_send.at[w], fd_recv.at[w * F + src, q], (g, z, partner),
        )

    def fin_copy(q, src, m):
        return remote(
            fin.at[0, src, core, row_block(mirror(m)), columns(q)], rs2.at[src, m, :, columns(q)],
            fx_send.at[0], fx_recv.at[src, q * (half - 1) + m - 1],
            (g, z, 2 * mirror(m) + core),
        )

    def ret_copy(q, src, m, device):
        return remote(
            fin.at[1, src, core, row_block(mirror(m)), columns(q)], ret.at[m, src, :, columns(q)],
            ret_send.at[0], ret_recv.at[src, q * half + m], (g, device, 2 * mirror(m) + core),
        )

    def units(w, d, body):
        def run(*_):
            if d == 0:
                body(z)
                return
            if d in ("near", "far"):
                body(z + (1 if d == "far" else -1) * (1 - 2 * upside))
                return

            def step(s, carry):
                body(z + (2 * s - 1) * d)
                return carry

            lax.fori_loop(1 - lax.div(z + F - d, F), 1 + lax.div(2 * F - 1 - z - d, F), step, 0)

        (for_helpers if w else for_middle)(run)

    def down(w, q, *ds):
        def body(src):
            value = jnp.dot(hidden[w], gd[src, q], preferred_element_type=jnp.float32).astype(jnp.bfloat16)
            put_rows(fin.at[w, src], columns(q), value)
            fin_pair(w, q, src).start()

        for d in ds:
            with jax.named_scope(f"down{w}{q}{d}"):
                units(w, d, body)

    def pair(w, q, *ds):
        def body(src):
            fin_pair(w, q, src).wait_recv()
            for m in range(1 - w, half):
                at = row_block(mirror(m))
                total = fin[w, src, core, at, columns(q)].astype(jnp.float32) + fpr[w, src, at, columns(q)].astype(jnp.float32)
                fin[w, src, core, at, columns(q)] = total.astype(jnp.bfloat16)
                if w:
                    for_helpers(lambda device: ret_copy(q, src, m, device).start())
                else:
                    fin_copy(q, src, m).start()

        for d in ds:
            with jax.named_scope(f"pair{w}{q}{d}"):
                units(w, d, body)

    def finish(q, *ds):
        def body(src):
            for m in range(1, half):
                fin_copy(q, src, m).wait_recv()
            at = row_block(chip)
            total = fin[0, src, core, at, columns(q)].astype(jnp.float32) + fpr[0, src, at, columns(q)].astype(jnp.float32)
            for m in range(1, half):
                total = total + rs2[src, m, :, columns(q)].astype(jnp.float32)
            cols = pl.ds(mult(src * N + q * GC, GC), GC)
            out[:, cols] = (resid[:, cols] + total).astype(jnp.bfloat16)

        for d in ds:
            with jax.named_scope(f"fin{q}{d}"):
                units(0, d, body)

    first_cols, last = range(G - 1), G - 1
    for q in range(G):
        down(0, q, 0)
    for q in range(G):
        pair(0, q, 0)
    service(7, *far)
    service(8, 1, side="near")
    mid(10)
    service(9, 1, side="far")
    for c in early:
        y_wait(c, 1, side="far")
    for q in first_cols:
        down(0, q, "far")
    with jax.named_scope("gpass1"):
        for_helpers(lambda device: gather_pass(1))
    service(9, 1, side="near")
    service(8, *far)
    for q in first_cols:
        pair(0, q, "far")
    with jax.named_scope("gwait1"):
        for_helpers(lambda device: gather_wait(1))

    def up_end(lo, hi):
        def body(device):
            def step(j, carry):
                up_block(1, j)
                return carry

            lax.fori_loop(lo, hi, step, 0)

        with jax.named_scope("up_end"):
            for_helpers(body)

    up_end(0, PIECES)
    service(10, 1, side="far")
    for q in range(G):
        down(1, q, 0)
    for q in first_cols:
        down(1, q, "far")
    for q in range(G):
        pair(1, q, 0)
    for q in first_cols:
        pair(1, q, "far")
    service(10, 1, side="near")
    for c in early:
        y_wait(c, *far)
    for q in first_cols:
        down(1, q, *far)
        down(0, q, *far)
    service(9, *far)
    for q in first_cols:
        pair(1, q, *far)
        pair(0, q, *far)
    for c in early:
        y_wait(c, 1, side="near")
    for q in first_cols:
        down(1, q, "near")
        down(0, q, "near")
    service(10, *far)
    for q in first_cols:
        pair(1, q, "near")
        pair(0, q, "near")
    for c in late:
        y_wait(c, 1, side="far")
    down(1, last, "far")
    down(0, last, "far")
    pair(1, last, "far")
    pair(0, last, "far")
    for q in range(G):
        finish(q, 0)
    for q in first_cols:
        finish(q, "far", *far)
        finish(q, "near")
    for c in late:
        y_wait(c, 1, side="near")
    down(1, last, "near")
    down(0, last, "near")
    pair(1, last, "near")
    pair(0, last, "near")
    finish(last, "far")
    for c in late:
        y_wait(c, *far)
    down(1, last, *far)
    down(0, last, *far)
    pair(1, last, *far)
    pair(0, last, *far)
    for c in order[-RING:]:
        drain(c)
    finish(last, "near", *far)

    def take(helper, left):
        for q in range(G):
            def step(src, carry):
                cols = pl.ds(mult(src * N + q * GC, GC), GC)
                total = resid[:, cols]
                for m in range(half):
                    ret_copy(q, src, m, helper).wait_recv()
                    total = total + ret[m, src, :, columns(q)].astype(jnp.float32)
                out[:, cols] = total.astype(jnp.bfloat16)
                return carry

            lax.fori_loop(0, F, step, 0)

    with jax.named_scope("take"):
        for_ends(take)

    for_ends(lambda helper, left: give_copy(helper).wait_send())
    def all_sent(ref, sem):
        remote(ref, ref, sem, sem, (other, z, t)).wait_send()

    all_sent(st_recv.at[1:T], st_send.at[0])
    all_sent(pr, md_send.at[0])
    all_sent(rs.at[1:half], mx_send.at[0])

    def layer_sent(w):
        all_sent(rs.at[1:half], agx_send.at[w])
        all_sent(rs, agd_send.at[w])
        all_sent(fpr.at[w], fd_send.at[w])
        if w:
            all_sent(ret, ret_send.at[0])
        else:
            all_sent(rs2.at[:, 1:half], fx_send.at[0])

    for_middle(lambda: layer_sent(0))
    for_helpers(lambda device: layer_sent(1))


def solution(mesh):
    F, T = mesh.shape["fs"], mesh.shape["tp"]

    def step(tokens, norm_in, w_value, w_gate, conv_kernel, ln_gain, ln_shift, w_out, norm_mlp, w_up, w_down):
        S, D = tokens.shape
        R, C = w_value.shape
        H = w_up.shape[1]
        N = w_out.shape[1]
        rows, half, G = S // T, T // 2, groups_of(N)
        chunks = 4 + 2 * PIECES
        bf16, f32 = jnp.bfloat16, jnp.float32
        dma = pltpu.SemaphoreType.DMA
        vmem = pl.BlockSpec(memory_space=pltpu.VMEM)
        anywhere = pl.BlockSpec(memory_space=pl.ANY)
        return pl.pallas_call(
            functools.partial(kernel, F, T),
            out_shape=jax.ShapeDtypeStruct((rows, D), bf16),
            in_specs=[anywhere, vmem, anywhere, vmem, vmem, vmem] + [anywhere] * 5,
            out_specs=vmem,
            scratch_shapes=[
                pltpu.VMEM((S, D), bf16),
                pltpu.VMEM(conv_kernel.shape, f32),
                pltpu.VMEM((S, D), bf16),
                pltpu.VMEM((D, C), bf16),
                pltpu.VMEM((D, C), bf16),
                pltpu.VMEM((F, C, N), bf16),
                pltpu.VMEM((PIECES, D, H // PIECES), bf16),
                pltpu.VMEM((F, G, H, N // G), bf16),
                pltpu.VMEM((S + PAD, C), f32),
                pltpu.VMEM((S, C), f32),
                pltpu.VMEM((S, C), bf16),
                pltpu.VMEM((2, half * rows, D), bf16),
                pltpu.VMEM((half * rows, D), bf16),
                pltpu.VMEM((half, rows, D), bf16),
                pltpu.VMEM((rows, D), f32),
                pltpu.VMEM((2, S, D), bf16),
                pltpu.VMEM((2, S, H), bf16),
                pltpu.VMEM((2, F, 2, half * rows, N), bf16),
                pltpu.VMEM((2, F, half * rows, N), bf16),
                pltpu.VMEM((F, half, rows, N), bf16),
                pltpu.VMEM((half, F, rows, N), bf16),
                pltpu.VMEM((8, S), f32),
                pltpu.VMEM((T, 8, S), f32),
                pltpu.VMEM((rows, D), bf16),
                dma((5 + PIECES + G,)),
            ]
            + [dma((RING, 2)), dma((RING,))]
            + [dma((RING, F - 1)), dma((chunks, F - 1)), dma((RING, F - 1)), dma((PIECES, F - 1)), dma((chunks - PIECES,))]
            + [dma((1,)), dma((T,)), dma((1,)), dma((F,)), dma((1,)), dma((F, half - 1))]
            + [dma((2,)), dma((2, half)), dma((2,)), dma((2, half - 1)), dma((2,))]
            + [dma((2,)), dma((2 * F, G)), dma((1,)), dma((F, G * (half - 1))), dma((1,)), dma((F, G * half))],
            compiler_params=pltpu.CompilerParams(
                collective_id=0, has_side_effects=True, vmem_limit_bytes=62 * 1024 * 1024
            ),
        )(
            tokens, norm_in, conv_kernel, ln_gain, ln_shift, norm_mlp, w_value, w_gate, w_out, w_up, w_down,
        )

    in_specs = (
        P(("grp", "fs"), None), P(), P("fs", "tp"), P("fs", "tp"), P(), P(), P(),
        P("tp", "fs"), P(), P("fs", "tp"), P("tp", "fs"),
    )
    return jax.shard_map(
        step, mesh=mesh, in_specs=in_specs, out_specs=P(("grp", "fs", "tp"), None), check_vma=False
    )
```

```python
import functools

import jax
import jax.numpy as jnp
from jax import lax
from jax.experimental import pallas as pl
from jax.experimental.pallas import tpu as pltpu
from jax.sharding import PartitionSpec as P

MESH = pl.DeviceIdType.MESH
PIECES = 4
PAD = 32
RING = 6


def rms_rows(x, gain):
    return x * lax.rsqrt(jnp.mean(x * x, axis=-1, keepdims=True) + 1e-06) * gain


def groups_of(n):
    return 2 if n >= 512 else 1


def early_shape(f, s, n):
    shape = (2, f, s, n // groups_of(n))
    return shape if 4 * 2 * f * s * shape[3] <= 4 * 1024 * 1024 else (2, 1, 8, 128)


def kernel(
    F, T,
    tok_h, norm_in, conv_h, ln_gain, ln_shift, norm_mlp, wv, wg, wo, wu, wd,
    out,
    tok, conv_k, normed, gv, gg, go, gu, gd, gated, conv, act, part, pr, rs, resid, nm, hidden, fin, fpr, rs2,
    held, ret, st_own, st_recv, nm_own,
    local_sem, own_sem, rest_sem, zsend, zrecv, ysend, yrecv, yrecv_all, st_send, st_rsem, md_send, md_recv, mx_send, mx_recv,
    agd_send, agd_recv, agx_send, agx_recv, give_sem, fd_send, fd_recv, fx_send, fx_recv, ret_send, ret_recv,
):
    g = lax.axis_index("grp")
    z = lax.axis_index("fs")
    t = lax.axis_index("tp")
    S, D = tok.shape
    R, C = wv.shape
    H = wu.shape[1]
    N = wo.shape[1]
    taps = conv_k.shape[0]
    rows = S // T
    half = T // 2
    R2, R4, C2, H2 = R // 2, R // 4, C // 2, H // 2
    HB = H // PIECES
    G = groups_of(N)
    subs = PIECES // G
    GC, HC = N // G, H2 // subs
    other = 1 - g
    n_chunks = 3 + 2 * PIECES
    first_down = 3 + PIECES
    early = range(first_down, first_down + subs * (G - 1))
    late = range(first_down + subs * (G - 1), n_chunks)
    second = n_chunks
    core = lax.rem(t, 2)
    chip = lax.div(t, 2)
    partner = t + 1 - 2 * core

    at_left, at_right = z == 0, z == F - 1
    is_end = jnp.logical_or(at_left, at_right)
    not_end = jnp.logical_not(is_end)
    help_left, help_right = z == 1, z == F - 2

    def upper(c):
        return int(3 <= c < n_chunks)

    def has_rest(c):
        return c >= 1

    def when_right(c):
        return pl.when(z < F - 1 - upper(c))

    def when_left(c):
        return pl.when(z > 0 + upper(c))

    def for_ends(body):
        @pl.when(at_left)
        def _():
            body(z + 1, 0)

        @pl.when(at_right)
        def _():
            body(z - 1, 1)

    def for_helpers(body):
        @pl.when(help_left)
        def _():
            body(z - 1)

        @pl.when(help_right)
        def _():
            body(z + 1)

    def for_middle(body):
        @pl.when(not_end)
        def _():
            body()

    def mult(i, k):
        return pl.multiple_of(i, k)

    def own(c, h):
        if c in (0, second):
            return wv.at[pl.ds(mult(h * R2 + (R4 if c else 0), R4), R4), :]
        if c < 3:
            ref, size = ((wv, R2), (wg, R2), (wo, C2))[c]
            return ref.at[pl.ds(mult(h * size, size), size), :]
        if c < first_down:
            return wu.at[pl.ds(mult(h * R2, R2), R2), pl.ds((c - 3) * HB, HB)]
        q, r = divmod(c - first_down, subs)
        return wd.at[pl.ds(mult(h * H2 + r * HC, HC), HC), pl.ds(q * GC, GC)]

    def slot(c, src, h):
        if c in (0, second):
            return gv.at[pl.ds(mult(src * R + h * R2 + (R4 if c else 0), R4), R4), :]
        if c < 2:
            return gg.at[pl.ds(mult(src * R + h * R2, R2), R2), :]
        if c == 2:
            return go.at[src, pl.ds(mult(h * C2, C2), C2), :]
        if c < first_down:
            return gu.at[c - 3, pl.ds(mult(src * R + h * R2, R2), R2), :]
        q, r = divmod(c - first_down, subs)
        return gd.at[src, q, pl.ds(mult(h * H2 + r * HC, HC), HC), :]

    def remote(src_ref, dst_ref, send, recv, device):
        return pltpu.make_async_remote_copy(
            src_ref=src_ref, dst_ref=dst_ref, send_sem=send, recv_sem=recv,
            device_id=device, device_id_type=MESH,
        )

    loads = [
        pltpu.make_async_copy(tok_h, tok, local_sem.at[0]),
        pltpu.make_async_copy(conv_h, conv_k, local_sem.at[1]),
    ]
    for copy in loads:
        copy.start()

    peers = [lax.rem(t + i, T) for i in range(T)]
    barrier = pltpu.get_barrier_semaphore()

    def greet(device):
        pl.semaphore_signal(barrier, inc=1, device_id=device, device_id_type=MESH)

    greet((other, z, t))
    for i in range(1, T):
        greet((g, z, peers[i]))

    @pl.when(z > 0)
    def _():
        greet((g, z - 1, t))

    @pl.when(z < F - 1)
    def _():
        greet((g, z + 1, t))

    ends = lax.div(z + F - 1, F) + lax.div(2 * F - 2 - z, F)
    def greet_mirrors(there):
        for m in range(1, half):
            greet((g, there, 2 * lax.rem(chip + m, half) + core))

    for_ends(lambda helper, left: greet_mirrors(helper))
    for_helpers(greet_mirrors)
    outer = lax.div(F + 1 - z, F) + lax.div(z + 2, F)
    with jax.named_scope("bar"):
        pl.semaphore_wait(barrier, T + ends + (half - 1) * outer)

    def index(d, left):
        return d - 1 if left else F - 1 - d

    order = (0, second, *range(1, n_chunks))

    def ring(c):
        return order.index(c) % RING

    def before(c):
        place = order.index(c) - RING
        return order[place] if place >= 0 else None

    def y_arrival(c, d, left):
        if c in early or c in late:
            return yrecv.at[c - first_down, index(d, left)]
        if c == 2:
            return yrecv.at[PIECES, index(d, left)]
        return yrecv_all.at[order.index(c)]

    def own_right(c):
        return remote(own(c, g), slot(c, z, g), own_sem.at[ring(c), 0], zrecv.at[c, index(1, 0)], (g, z + 1, t))

    def own_left(c):
        return remote(own(c, g), slot(c, z, g), own_sem.at[ring(c), 1], zrecv.at[c, index(1, 1)], (g, z - 1, t))

    def hop(c, d, src, left):
        here = slot(c, src, g)
        return remote(
            here, here, zsend.at[ring(c), index(d, left)], zrecv.at[c, index(d + 1, left)], (g, z - 1 if left else z + 1, t)
        )

    def arrival(c, d, src, left):
        here = slot(c, src, g)
        return remote(here, here, zsend.at[ring(c), index(d, left)], zrecv.at[c, index(d, left)], (other, z, t))

    def across(c, d, src, left, h=g):
        here = slot(c, src, h)
        return remote(here, here, ysend.at[ring(c), index(d, left)], y_arrival(c, d, left), (other, z, t))

    def own_rest(c, helper, left):
        return remote(own(c, other), slot(c, z, other), rest_sem.at[ring(c)], y_arrival(c, 1, left), (g, helper, t))

    low = z < F // 2
    high = jnp.logical_not(low)
    upside = lax.div(z, F // 2)

    def on_side(cond, left, side):
        if side is None:
            return cond
        return jnp.logical_and(cond, high if bool(left) == (side == "near") else low)

    def own_send(c, act_on, side=None):
        @pl.when(on_side(z < F - 1 - upper(c), 1, side))
        def _():
            act_on(own_right(c))

        @pl.when(on_side(z > 0 + upper(c), 0, side))
        def _():
            act_on(own_left(c))

    def start(copy):
        copy.start()

    def sent(copy):
        copy.wait_send()

    def mid(c, side=None):
        if before(c) is not None:
            for_middle(lambda: own_send(before(c), sent, side))
        for_middle(lambda: own_send(c, start, side))

    def rest_send(c, act_on):
        if has_rest(c):
            for_ends(lambda helper, left: act_on(own_rest(c, helper, left)))

    def end(c, first=True, rest=True):
        @pl.when(is_end)
        def _():
            if first:
                if before(c) is not None:
                    own_send(before(c), sent)
                own_send(c, start)
            if rest:
                if before(c) is not None:
                    rest_send(before(c), sent)
                rest_send(c, start)

    def both(d, body, c=0, side=None, who=None):
        def cond(base, left):
            base = on_side(base, left, side)
            return base if who is None else jnp.logical_and(base, is_end if who == "ends" else not_end)

        @pl.when(cond(jnp.logical_and(z - d >= 0, z < F - upper(c)), 0))
        def _():
            body(z - d, 0)

        @pl.when(cond(jnp.logical_and(z + d < F, z >= 0 + upper(c)), 1))
        def _():
            body(z + d, 1)

    def when_across(c, d, left):
        if d > 1 or not has_rest(c):
            return lambda body: body()
        return pl.when(z != (F - 2 if left else 1))

    def forward(c, d, src, left, act_on):
        if d < F - 1:
            @(when_left if left else when_right)(c)
            def _():
                act_on(hop(c, d, src, left))

        @when_across(c, d, left)
        def _():
            act_on(across(c, d, src, left))

    def service(c, *ds, side=None, who=None):
        for d in ds:
            with jax.named_scope(f"S{c}_{d}{side or ''}"):
                def body(src, left):
                    arrival(c, d, src, left).wait_recv()
                    forward(c, d, src, left, start)

                if before(c) is not None:
                    both(d, lambda src, left: forward(before(c), d, src, left, sent), before(c), side, who)
                both(d, body, c, side, who)

    every, far = range(1, F), range(2, F)

    def y_wait(c, *ds, side=None):
        for d in ds:
            with jax.named_scope(f"Y{c}_{d}{side or ''}"):
                def body(src, left):
                    across(c, d, src, left, other).wait_recv()

                both(d, body, c, side)

    def y_wait_all(c):
        if c in (0, second):
            got = gv.at[0 : (F - 1) * R4, :]
        elif c < 3:
            got = gg.at[0 : (F - 1) * R2, :]
        else:
            got = gu.at[c - 3, 0 : (F - 1) * R2, :]

        def body():
            remote(got, got, yrecv_all.at[order.index(c)], yrecv_all.at[order.index(c)], (other, z, t)).wait_recv()

        with jax.named_scope(f"Y{c}"):
            for_middle(body) if upper(c) else body()

    def drain(c):
        own_send(c, sent)
        rest_send(c, sent)
        for d in range(1, F):
            both(d, lambda src, left: forward(c, d, src, left, sent), c)

    for c in (0, second):
        mid(c)
        end(c, rest=False)
    mid(1, "near")
    end(1, rest=False)
    end(2, rest=False)
    copies = [
        pltpu.make_async_copy(wv, gv.at[pl.ds(mult(z * R, R), R), :], local_sem.at[2]),
        pltpu.make_async_copy(wg, gg.at[pl.ds(mult(z * R, R), R), :], local_sem.at[3]),
        pltpu.make_async_copy(wo, go.at[z], local_sem.at[4]),
    ]
    for j in range(PIECES):
        copies.append(
            pltpu.make_async_copy(
                wu.at[:, pl.ds(j * HB, HB)], gu.at[j, pl.ds(mult(z * R, R), R), :], local_sem.at[5 + j]
            )
        )
    for q in range(G):
        copies.append(pltpu.make_async_copy(wd.at[:, pl.ds(q * GC, GC)], gd.at[z, q], local_sem.at[5 + PIECES + q]))
    end(second, first=False)
    end(1, first=False)
    end(2, first=False)
    end(3)
    for copy in copies:
        copy.start()
    for copy in loads:
        copy.wait()

    block = 64

    def norm_step(i, carry):
        at = pl.ds(mult(i * block, block), block)
        x = tok[at, :].astype(jnp.float32)
        normed[at, :] = rms_rows(x, norm_in[...].reshape(1, D).astype(jnp.float32)).astype(jnp.bfloat16)
        return carry

    with jax.named_scope("norm"):
        lax.fori_loop(0, S // block, norm_step, 0)
    for copy in copies:
        copy.wait()

    service(0, 1)
    service(second, 1)
    mid(1, "far")
    service(1, 1, side="near")
    mid(2, "far")
    service(1, 1, who="ends")
    service(0, *far)
    service(second, *far)
    end(4)
    service(1, 1, side="far", who="middle")
    service(2, 1, side="near")
    mid(3)
    mid(4)
    service(1, *far)
    mid(2, "near")
    end(5)
    service(2, 1, side="far")
    y_wait_all(0)
    y_wait_all(second)
    y_wait_all(1)

    tile = min(256, C)
    gated[0:PAD, :] = jnp.zeros((PAD, C), jnp.float32)

    def gate_step(i, carry):
        at = pl.ds(mult(i * tile, tile), tile)
        v = jnp.dot(normed[...], gv[:, at], preferred_element_type=jnp.float32)
        a = jnp.dot(normed[...], gg[:, at], preferred_element_type=jnp.float32)
        gated[PAD:, at] = v * jax.nn.sigmoid(a)
        return carry

    with jax.named_scope("gate"):
        lax.fori_loop(0, C // tile, gate_step, 0)

    span = 128
    lead = PAD - (taps - 1)

    def conv_step(i, carry):
        base = mult(i * span, span)
        first = jnp.zeros((span, 128), jnp.float32)
        second = jnp.zeros((span, 128), jnp.float32)
        for j in range(C // 128):
            lanes = pl.ds(j * 128, 128)
            window = gated[pl.ds(base, span + PAD), lanes]
            weights = conv_k[:, pl.ds(mult(t * C + j * 128, 128), 128)]
            acc = jnp.zeros((span, 128), jnp.float32)
            for k in range(taps):
                acc = acc + weights[k : k + 1, :] * window[lead + k : lead + k + span, :]
            conv[pl.ds(base, span), lanes] = acc
            first = first + acc
            second = second + acc * acc
        lane = lax.broadcasted_iota(jnp.int32, (span, 128), 1)
        both_sums = jnp.where(
            lane == 0,
            jnp.sum(first, axis=1, keepdims=True),
            jnp.where(lane == 1, jnp.sum(second, axis=1, keepdims=True), 0.0),
        )
        st_own[:, pl.ds(base, span)] = jnp.transpose(both_sums)[0:8, :]
        return carry

    spans = S // span
    end(6, rest=False)
    service(2, *far, who="middle")
    with jax.named_scope("conv_a"):
        lax.fori_loop(0, spans // 2, conv_step, 0)
    service(3, 1, side="near")
    mid(5)
    service(3, 1, side="far")
    service(2, 2, who="ends")
    with jax.named_scope("conv_b"):
        lax.fori_loop(spans // 2, spans, conv_step, 0)

    def stat_copy(i):
        return remote(st_own, st_recv.at[i], st_send.at[0], st_rsem.at[i], (g, z, peers[i]))

    for i in range(1, T):
        stat_copy(i).start()
    service(2, *far[1:], who="ends")
    service(4, 1, side="far")
    service(4, 1, side="near")
    mid(6)
    for i in range(1, T):
        stat_copy(i).wait_recv()

    gain = ln_gain[pl.ds(mult(t * C, C), C)].reshape(1, C).astype(jnp.float32)
    shift = ln_shift[pl.ds(mult(t * C, C), C)].reshape(1, C).astype(jnp.float32)

    def act_step(i, carry):
        base = mult(i * span, span)
        at = pl.ds(base, span)
        sums = st_own[:, at]
        for k in range(1, T):
            sums = sums + st_recv[k, :, at]
        mean = sums[0:1, :] / D
        var = sums[1:2, :] / D - mean * mean
        scale = lax.rsqrt(var + 1e-05)
        mean_c = jnp.transpose(jnp.broadcast_to(mean, (128, span)))[:, 0:1]
        scale_c = jnp.transpose(jnp.broadcast_to(scale, (128, span)))[:, 0:1]
        n = (conv[at, :] - mean_c) * scale_c * gain + shift
        act[at, :] = (n * jax.nn.sigmoid(n)).astype(jnp.bfloat16)
        return carry

    with jax.named_scope("act"):
        lax.fori_loop(0, S // span, act_step, 0)

    def put_rows(ref, cols, value):
        for r in range(T):
            ref[r % 2, (r // 2) * rows : (r // 2 + 1) * rows, cols] = value[r * rows : (r + 1) * rows, :]

    def row_block(j):
        return pl.ds(mult(j * rows, rows), rows)

    def mirror(i):
        return lax.rem(chip + i, half)

    def mirror_source(i):
        return lax.rem(chip - i + half, half)

    def mix_pair(i):
        cols = pl.ds(mult(i * N, N), N)
        return remote(part.at[1 - core, :, cols], pr.at[:, cols], md_send.at[0], md_recv.at[i], (g, z, partner))

    def mix_copy(i, m):
        cols = pl.ds(mult(i * N, N), N)
        return remote(
            part.at[core, row_block(mirror(m)), cols], rs.at[m, :, cols], mx_send.at[0], mx_recv.at[i, m - 1],
            (g, z, 2 * mirror(m) + core),
        )

    def sources(d, body):
        if d == 0:
            body(z)
            return

        def step(s, carry):
            body(z + (2 * s - 1) * d)
            return carry

        lax.fori_loop(1 - lax.div(z + F - d, F), 1 + lax.div(2 * F - 1 - z - d, F), step, 0)

    def out_block(i):
        value = jnp.dot(act[...], go[i], preferred_element_type=jnp.float32).astype(jnp.bfloat16)
        put_rows(part, pl.ds(mult(i * N, N), N), value)
        mix_pair(i).start()

    def pair_block(i):
        mix_pair(i).wait_recv()
        cols = pl.ds(mult(i * N, N), N)
        for m in range(1, half):
            at = row_block(mirror(m))
            total = part[core, at, cols].astype(jnp.float32) + pr[at, cols].astype(jnp.float32)
            part[core, at, cols] = total.astype(jnp.bfloat16)
            mix_copy(i, m).start()

    for d in range(F):
        if d:
            y_wait(2, d)
        with jax.named_scope(f"outp{d}"):
            sources(d, out_block)
        if d:
            with jax.named_scope(f"mixpair{d - 1}"):
                sources(d - 1, pair_block)
    with jax.named_scope(f"mixpair{F - 1}"):
        sources(F - 1, pair_block)
    service(3, *far)
    service(5, 1, side="far")
    service(5, 1, side="near")
    mid(7)

    def mix_wait(i, carry):
        for m in range(1, half):
            mix_copy(i, m).wait_recv()
        return carry

    with jax.named_scope("mixw"):
        lax.fori_loop(0, F, mix_wait, 0)

    small = 32

    def resid_step(i, carry):
        at = pl.ds(mult(i * small, small), small)
        mine = pl.ds(mult(t * rows + i * small, small), small)
        kept = pl.ds(mult(chip * rows + i * small, small), small)
        total = part[core, kept, :].astype(jnp.float32) + pr[kept, :].astype(jnp.float32)
        for m in range(1, half):
            total = total + rs[m, at, :].astype(jnp.float32)
        r = tok[mine, :].astype(jnp.float32) + total
        resid[at, :] = r
        nm_own[at, :] = rms_rows(r, norm_mlp[...].reshape(1, D).astype(jnp.float32)).astype(jnp.bfloat16)
        return carry

    with jax.named_scope("resid"):
        lax.fori_loop(0, rows // small, resid_step, 0)
    mine = row_block(t)

    def give_copy(helper):
        return remote(nm_own, nm.at[1, mine, :], give_sem.at[0], give_sem.at[1], (g, helper, t))

    for_ends(lambda helper, left: give_copy(helper).start())
    end(7, rest=False)
    end(6, first=False)
    end(8, rest=False)
    end(9, rest=False)
    end(7, first=False)
    end(10, rest=False)
    for c in range(8, n_chunks):
        end(c, first=False)

    def gather_x(w, i):
        src = nm_own if w == 0 else nm.at[w, mine, :]
        return remote(src, nm.at[w, mine, :], agx_send.at[w], agx_recv.at[w, i - 1], (g, z, 2 * mirror(i) + core))

    def gather_x_arrival(w, i):
        there = row_block(2 * mirror_source(i) + core)
        return remote(nm.at[w, there, :], nm.at[w, there, :], agx_send.at[w], agx_recv.at[w, i - 1], (g, z, partner))

    def gather_d(w, i):
        if i == 0:
            src = nm_own if w == 0 else nm.at[w, mine, :]
            return remote(src, nm.at[w, mine, :], agd_send.at[w], agd_recv.at[w, 0], (g, z, partner))
        there = row_block(2 * mirror_source(i) + core)
        return remote(nm.at[w, there, :], nm.at[w, there, :], agd_send.at[w], agd_recv.at[w, i], (g, z, partner))

    def gather_d_arrival(w, i):
        there = row_block(2 * mirror_source(i) + 1 - core)
        return remote(nm.at[w, there, :], nm.at[w, there, :], agd_send.at[w], agd_recv.at[w, i], (g, z, partner))

    def gather_start(w):
        for i in range(1, half):
            gather_x(w, i).start()
        gather_d(w, 0).start()

    def gather_pass(w):
        for i in range(1, half):
            gather_x_arrival(w, i).wait_recv()
            gather_d(w, i).start()

    def gather_wait(w):
        for i in range(half):
            gather_d_arrival(w, i).wait_recv()

    def gather_first():
        gather_start(0)
        nm[0, mine, :] = nm_own[...]

    for_middle(gather_first)
    service(4, *far)
    service(6, 1, side="far")
    service(6, 1, side="near")
    mid(8)
    service(5, *far)
    with jax.named_scope("gpass0"):
        for_middle(lambda: gather_pass(0))
    service(7, 1, side="far")
    mid(9)
    with jax.named_scope("gwait0"):
        for_middle(lambda: gather_wait(0))

    utile = min(256, HB)

    def up_block(w, j):
        def up_step(i, carry):
            at = pl.ds(mult(i * utile, utile), utile)
            a = jnp.dot(nm[w], gu[j, :, at], preferred_element_type=jnp.float32)
            a = jnp.maximum(a, 0.0)
            hidden[w, :, pl.ds(mult(j * HB + i * utile, utile), utile)] = (a * a).astype(jnp.bfloat16)
            return carry

        lax.fori_loop(0, HB // utile, up_step, 0)

    def up(j):
        y_wait_all(3 + j)
        with jax.named_scope(f"up{j}"):
            for_middle(lambda: up_block(0, j))

    up(0)

    def share(device):
        remote(nm_own, nm.at[1, mine, :], give_sem.at[0], give_sem.at[1], (g, device, t)).wait_recv()
        gather_start(1)

    with jax.named_scope("share"):
        for_helpers(share)
    up(1)
    service(6, *far)
    up(2)
    service(7, 1, side="near")
    service(8, 1, side="far")
    up(3)
    with jax.named_scope("gpass1"):
        for_helpers(lambda device: gather_pass(1))
    service(9, 1, side="far")

    def columns(q):
        return pl.ds(q * GC, GC)

    def fin_pair(w, q, src):
        return remote(
            fin.at[w, src, 1 - core, :, columns(q)], fpr.at[w, src, :, columns(q)],
            fd_send.at[w], fd_recv.at[w * F + src, q], (g, z, partner),
        )

    def fin_copy(q, src, m):
        return remote(
            fin.at[0, src, core, row_block(mirror(m)), columns(q)], rs2.at[src, m, :, columns(q)],
            fx_send.at[0], fx_recv.at[src, q * (half - 1) + m - 1],
            (g, z, 2 * mirror(m) + core),
        )

    def ret_copy(q, src, m, device):
        return remote(
            fin.at[1, src, core, row_block(mirror(m)), columns(q)], ret.at[m, src, :, columns(q)],
            ret_send.at[0], ret_recv.at[src, q * half + m], (g, device, 2 * mirror(m) + core),
        )

    def units(w, d, body):
        def run(*_):
            if d in ("near", "far"):
                body(z + (1 if d == "far" else -1) * (1 - 2 * upside))
            else:
                sources(d, body)

        (for_helpers if w else for_middle)(run)

    def down(w, q, *ds):
        def body(src):
            value = jnp.dot(hidden[w], gd[src, q], preferred_element_type=jnp.float32).astype(jnp.bfloat16)
            put_rows(fin.at[w, src], columns(q), value)
            fin_pair(w, q, src).start()

        for d in ds:
            with jax.named_scope(f"down{w}{q}{d}"):
                units(w, d, body)

    tail = pl.ds(mult(other * H2 + (subs - 1) * HC, HC), HC)

    starts_early = held.shape[1] == F

    def down_part(w, *ds):
        if not starts_early:
            return

        def body(src):
            at = pl.ds(mult(g * H2, H2), H2)
            total = jnp.dot(hidden[w, :, at], gd[src, G - 1, at, :], preferred_element_type=jnp.float32)
            if subs > 1:
                at = pl.ds(mult(other * H2, H2), (subs - 1) * HC)
                total = total + jnp.dot(hidden[w, :, at], gd[src, G - 1, at, :], preferred_element_type=jnp.float32)
            held[w, src] = total

        for d in ds:
            with jax.named_scope(f"dpart{w}{d}"):
                units(w, d, body)

    def down_rest(w, *ds):
        if not starts_early:
            down(w, G - 1, *ds)
            return

        def body(src):
            total = held[w, src] + jnp.dot(hidden[w, :, tail], gd[src, G - 1, tail, :], preferred_element_type=jnp.float32)
            put_rows(fin.at[w, src], columns(G - 1), total.astype(jnp.bfloat16))
            fin_pair(w, G - 1, src).start()

        for d in ds:
            with jax.named_scope(f"drest{w}{d}"):
                units(w, d, body)

    def pair(w, q, *ds):
        def body(src):
            fin_pair(w, q, src).wait_recv()
            for m in range(1 - w, half):
                at = row_block(mirror(m))
                total = fin[w, src, core, at, columns(q)].astype(jnp.float32) + fpr[w, src, at, columns(q)].astype(jnp.float32)
                fin[w, src, core, at, columns(q)] = total.astype(jnp.bfloat16)
                if w:
                    for_helpers(lambda device: ret_copy(q, src, m, device).start())
                else:
                    fin_copy(q, src, m).start()

        for d in ds:
            with jax.named_scope(f"pair{w}{q}{d}"):
                units(w, d, body)

    def finish(q, *ds):
        def body(src):
            for m in range(1, half):
                fin_copy(q, src, m).wait_recv()
            at = row_block(chip)
            total = fin[0, src, core, at, columns(q)].astype(jnp.float32) + fpr[0, src, at, columns(q)].astype(jnp.float32)
            for m in range(1, half):
                total = total + rs2[src, m, :, columns(q)].astype(jnp.float32)
            cols = pl.ds(mult(src * N + q * GC, GC), GC)
            out[:, cols] = (resid[:, cols] + total).astype(jnp.bfloat16)

        for d in ds:
            with jax.named_scope(f"fin{q}{d}"):
                units(0, d, body)

    first_cols, last = range(G - 1), G - 1
    for q in range(G):
        down(0, q, 0)
    service(7, *far)
    for q in range(G):
        pair(0, q, 0)
    service(8, 1, side="near")
    mid(10)
    with jax.named_scope("gwait1"):
        for_helpers(lambda device: gather_wait(1))

    def up_end(lo, hi):
        def body(device):
            def step(j, carry):
                up_block(1, j)
                return carry

            lax.fori_loop(lo, hi, step, 0)

        with jax.named_scope("up_end"):
            for_helpers(body)

    up_end(0, PIECES)
    service(8, *far)
    for q in range(G):
        down(1, q, 0)
    service(9, 1, side="near")
    for q in range(G):
        pair(1, q, 0)
    for c in early:
        y_wait(c, 1, side="far")
    for q in first_cols:
        down(1, q, "far")
        down(0, q, "far")
    service(10, 1, side="far")
    for q in first_cols:
        pair(1, q, "far")
        pair(0, q, "far")
    service(10, 1, side="near")
    for c in early:
        y_wait(c, *far)
    for q in first_cols:
        down(1, q, *far)
        down(0, q, *far)
    service(9, *far)
    for q in first_cols:
        pair(1, q, *far)
        pair(0, q, *far)
    for c in early:
        y_wait(c, 1, side="near")
    for q in first_cols:
        down(1, q, "near")
        down(0, q, "near")
    service(10, *far)
    for q in first_cols:
        pair(1, q, "near")
        pair(0, q, "near")
    for c in late:
        y_wait(c, 1, side="far")
    down(1, last, "far")
    down(0, last, "far")
    pair(1, last, "far")
    pair(0, last, "far")
    for c in late[:-1]:
        y_wait(c, 1, side="near")
    down_part(1, "near")
    down_part(0, "near")
    for q in range(G):
        finish(q, 0)
    for c in late[:-1]:
        y_wait(c, *far)
    down_part(1, *far)
    down_part(0, *far)
    for q in first_cols:
        finish(q, "far", *far)
        finish(q, "near")
    y_wait(late[-1], 1, side="near")
    down_rest(1, "near")
    down_rest(0, "near")
    pair(1, last, "near")
    pair(0, last, "near")
    finish(last, "far")
    y_wait(late[-1], *far)
    down_rest(1, *far)
    down_rest(0, *far)
    pair(1, last, *far)
    pair(0, last, *far)
    for c in order[-RING:]:
        drain(c)
    finish(last, "near", *far)

    def take(helper, left):
        for q in range(G):
            def step(src, carry):
                cols = pl.ds(mult(src * N + q * GC, GC), GC)
                total = resid[:, cols]
                for m in range(half):
                    ret_copy(q, src, m, helper).wait_recv()
                    total = total + ret[m, src, :, columns(q)].astype(jnp.float32)
                out[:, cols] = total.astype(jnp.bfloat16)
                return carry

            lax.fori_loop(0, F, step, 0)

    with jax.named_scope("take"):
        for_ends(take)

    for_ends(lambda helper, left: give_copy(helper).wait_send())
    def all_sent(ref, sem):
        remote(ref, ref, sem, sem, (other, z, t)).wait_send()

    all_sent(st_recv.at[1:T], st_send.at[0])
    all_sent(pr, md_send.at[0])
    all_sent(rs.at[1:half], mx_send.at[0])

    def layer_sent(w):
        all_sent(rs.at[1:half], agx_send.at[w])
        all_sent(rs, agd_send.at[w])
        all_sent(fpr.at[w], fd_send.at[w])
        if w:
            all_sent(ret, ret_send.at[0])
        else:
            all_sent(rs2.at[:, 1:half], fx_send.at[0])

    for_middle(lambda: layer_sent(0))
    for_helpers(lambda device: layer_sent(1))


def solution(mesh):
    F, T = mesh.shape["fs"], mesh.shape["tp"]

    def step(tokens, norm_in, w_value, w_gate, conv_kernel, ln_gain, ln_shift, w_out, norm_mlp, w_up, w_down):
        S, D = tokens.shape
        R, C = w_value.shape
        H = w_up.shape[1]
        N = w_out.shape[1]
        rows, half, G = S // T, T // 2, groups_of(N)
        chunks = 4 + 2 * PIECES
        bf16, f32 = jnp.bfloat16, jnp.float32
        dma = pltpu.SemaphoreType.DMA
        vmem = pl.BlockSpec(memory_space=pltpu.VMEM)
        anywhere = pl.BlockSpec(memory_space=pl.ANY)
        return pl.pallas_call(
            functools.partial(kernel, F, T),
            out_shape=jax.ShapeDtypeStruct((rows, D), bf16),
            in_specs=[anywhere, vmem, anywhere, vmem, vmem, vmem] + [anywhere] * 5,
            out_specs=vmem,
            scratch_shapes=[
                pltpu.VMEM((S, D), bf16),
                pltpu.VMEM(conv_kernel.shape, f32),
                pltpu.VMEM((S, D), bf16),
                pltpu.VMEM((D, C), bf16),
                pltpu.VMEM((D, C), bf16),
                pltpu.VMEM((F, C, N), bf16),
                pltpu.VMEM((PIECES, D, H // PIECES), bf16),
                pltpu.VMEM((F, G, H, N // G), bf16),
                pltpu.VMEM((S + PAD, C), f32),
                pltpu.VMEM((S, C), f32),
                pltpu.VMEM((S, C), bf16),
                pltpu.VMEM((2, half * rows, D), bf16),
                pltpu.VMEM((half * rows, D), bf16),
                pltpu.VMEM((half, rows, D), bf16),
                pltpu.VMEM((rows, D), f32),
                pltpu.VMEM((2, S, D), bf16),
                pltpu.VMEM((2, S, H), bf16),
                pltpu.VMEM((2, F, 2, half * rows, N), bf16),
                pltpu.VMEM((2, F, half * rows, N), bf16),
                pltpu.VMEM((F, half, rows, N), bf16),
                pltpu.VMEM(early_shape(F, S, N), f32),
                pltpu.VMEM((half, F, rows, N), bf16),
                pltpu.VMEM((8, S), f32),
                pltpu.VMEM((T, 8, S), f32),
                pltpu.VMEM((rows, D), bf16),
                dma((5 + PIECES + G,)),
            ]
            + [dma((RING, 2)), dma((RING,))]
            + [dma((RING, F - 1)), dma((chunks, F - 1)), dma((RING, F - 1)), dma((PIECES + 1, F - 1)), dma((chunks - PIECES,))]
            + [dma((1,)), dma((T,)), dma((1,)), dma((F,)), dma((1,)), dma((F, half - 1))]
            + [dma((2,)), dma((2, half)), dma((2,)), dma((2, half - 1)), dma((2,))]
            + [dma((2,)), dma((2 * F, G)), dma((1,)), dma((F, G * (half - 1))), dma((1,)), dma((F, G * half))],
            compiler_params=pltpu.CompilerParams(
                collective_id=0, has_side_effects=True, vmem_limit_bytes=63 * 1024 * 1024
            ),
        )(
            tokens, norm_in, conv_kernel, ln_gain, ln_shift, norm_mlp, w_value, w_gate, w_out, w_up, w_down,
        )

    in_specs = (
        P(("grp", "fs"), None), P(), P("fs", "tp"), P("fs", "tp"), P(), P(), P(),
        P("tp", "fs"), P(), P("fs", "tp"), P("tp", "fs"),
    )
    return jax.shard_map(
        step, mesh=mesh, in_specs=in_specs, out_specs=P(("grp", "fs", "tp"), None), check_vma=False
    )
```
